32 devices in a mesh: ep: 8 (over z, x), tp: 4 (over y, core).
Axes of the slice: x: 2, y: 2, z: 4, core: 2. Of those that a mesh axis runs over, the one named last changes fastest.
Arguments:
- x_in: bfloat16 [4096, 3072], P('tp', 'ep'), may hold values from -6 to 6
- z_in: bfloat16 [4096, 3072], P('tp', 'ep'), may hold values from -6 to 6
- dt_raw: float32 [64, 3072], P('tp', 'ep'), may hold values from -6 to 6
- decay_rate: float32 [64], P('tp'), may hold values from 0 to 1, as said below
- b_in: bfloat16 [256, 3072], P(None, 'ep'), may hold values from -6 to 6
- c_in: bfloat16 [256, 3072], P(None, 'ep'), may hold values from -6 to 6
- conv_x: float32 [4096, 4], P('tp'), may hold values from -3 to 3
- conv_b: float32 [256, 4], replicated, may hold values from -3 to 3
- conv_c: float32 [256, 4], replicated, may hold values from -3 to 3
- head_gain: float32 [4096], P('tp'), may hold values from 0.1 to 1.9
- moe_rows: bfloat16 [1280, 2048], P('ep'), may hold values from -6 to 6
- moe_gain: float32 [2048], replicated, may hold values from 0.1 to 1.9
- routes: int32 [1280, 2], P('ep'), may hold values from 0 to 7, all different within a row; in each aligned block of 160 rows (0 to 159, 160 to 319, ...) at most 80 rows name the same one
- route_logit: float32 [1280, 2], P('ep'), may hold values from -6 to 6
- w_gate: bfloat16 [8, 2048, 5120], P('ep', None, 'tp'), may hold values from -0.125 to 0.125
- w_up: bfloat16 [8, 2048, 5120], P('ep', None, 'tp'), may hold values from -0.125 to 0.125
- w_down: bfloat16 [8, 5120, 2048], P('ep', 'tp'), may hold values from -0.078125 to 0.078125
Outputs:
- mixed: bfloat16 [4096, 3072], P('tp', 'ep')
- moe_out: bfloat16 [2048, 1280], P('tp', 'ep')
The draws below stay inside these ranges and needn't reach their ends.
Inputs may be any that keep to these rules, and one draw needn't show every extreme that they name: `routes`: each row names 2 different experts; among the rows of one index of ep no expert is named more than 80 times, a bound that some block reaches. `decay_rate`: positive rates.
All inputs are finite; a program needn't handle non-finite values.
Results may differ from the reference program's by a relative error of at most 0.018.
Values may be sent and summed in bfloat16 or wider, within the bound.
No kernel may reach another device: no remote copies, remote signals or barrier semaphores. Data moves between devices by JAX's collectives and lax.ppermute only.
A program may use at most 64 MiB of HBM per device.

```python
import math
import jax
import jax.numpy as jnp
import numpy as np
from jax import lax

D = 2048
HEADS = 64
HEAD_DIM = 64
GROUPS = 2
NSTATE = 128
KCONV = 4
BLOCK = 128
FF = 5120
TOP = 2
L_DEV = 384
MOE_DEV = 160
SEQLEN = 3072
MTOK = 1280
EXPERTS = 8
CAP = 80
N_EP = 8
N_TP = 4


def draw_decay_rate(key, part):
    order_key, slow_key, fast_key = jax.random.split(jax.random.fold_in(key, 11), 3)
    fast_count = HEADS // 2
    is_fast = jax.random.permutation(order_key, HEADS) < fast_count
    slow_rate = jnp.exp(jax.random.uniform(slow_key, (HEADS,), jnp.float32, math.log(0.05 / SEQLEN), math.log(1.0 / SEQLEN)))
    fast_rate = jnp.exp(jax.random.uniform(fast_key, (HEADS,), jnp.float32, math.log(0.012), math.log(0.04)))
    return jnp.where(is_fast, fast_rate, slow_rate)


def draw_dt_raw(key, part):
    noise_key, span_key, block_key = jax.random.split(jax.random.fold_in(key, 23), 3)
    noise = jnp.clip(0.7 * jax.random.normal(noise_key, (HEADS, SEQLEN), jnp.float32), -4.0, 4.0)
    span_shift = jax.random.uniform(span_key, (HEADS, SEQLEN // L_DEV), jnp.float32, -1.5, 1.5)
    block_shift = jax.random.uniform(block_key, (HEADS, SEQLEN // BLOCK), jnp.float32, -0.5, 0.5)
    return noise + jnp.repeat(span_shift, L_DEV, axis=1) + jnp.repeat(block_shift, BLOCK, axis=1)


def levels(stream_key, extent, pieces, smallest, largest):
    loudness, own = 1.0, jax.random.fold_in(stream_key, 6)
    for axis_at, shards_of in pieces:
        steps = jnp.exp(jax.random.uniform(jax.random.fold_in(own, axis_at), (shards_of,), jnp.float32, smallest / len(pieces), largest / len(pieces)))
        loudness = loudness * jnp.repeat(steps, extent[axis_at] // shards_of).reshape([-1 if axis == axis_at else 1 for axis in range(len(extent))])
    return loudness


def assign_block(stream_key, own, number, rows, amount, top, bound, lean):
    ranking = jax.random.permutation(stream_key, amount)
    crowded, usual = portions_of(amount, rows * top, bound, lean, True), portions_of(amount, rows * top, bound, lean, False)
    places = jnp.arange(amount)

    def named(sizes, rotation):
        used = int((sizes > 0).sum())
        fixed = max(1, used // 4)
        moved = fixed + (places - fixed + rotation * (used - fixed)) % max(1, amount - fixed)
        return jnp.zeros((amount,), jnp.int32).at[ranking[jnp.where(places < fixed, places, moved)]].set(jnp.asarray(sizes, jnp.int32))

    sizes = jnp.where(number % 4 == 0, named(crowded, number // 4), named(usual, number - number // 4 - 1))
    mixed = jax.random.permutation(jax.random.fold_in(own, 3), amount)
    giver, receiver = mixed[0:amount // 2 * 2:2], mixed[1:amount // 2 * 2:2]
    slack = jnp.minimum(sizes[giver] - 1, bound - sizes[receiver]) // 2
    slack = jnp.where((giver == ranking[0]) | (receiver == ranking[0]) | (sizes[receiver] == 0), 0, jnp.maximum(slack, 0))
    moved = jax.random.randint(jax.random.fold_in(own, 4), (amount // 2,), 0, 1 << 20) % (slack + 1)
    sizes = sizes.at[giver].add(-moved).at[receiver].add(moved)
    items = jnp.searchsorted(jnp.cumsum(sizes), jnp.arange(rows * top), side="right").astype(jnp.int32)
    grid = items.reshape(top, rows).T
    grid = grid[jax.random.permutation(jax.random.fold_in(own, 1), rows)]
    rotation = jax.random.randint(jax.random.fold_in(own, 2), (rows, 1), 0, top)
    return jnp.take_along_axis(grid, (jnp.arange(top)[None, :] + rotation) % top, axis=1)


def portions_of(amount, total, most, skew, full):
    loads = [(1 << 20) // math.isqrt(grade ** skew) + 1 for grade in range(1, amount + 1)]
    largest = most if full else min(most, max(-(-total // amount), total * loads[0] // sum(loads)))
    least = 1 if total - largest >= amount - 1 else 0
    given, spare = [largest] + [least] * (amount - 1), total - largest - least * (amount - 1)
    while spare > 0:
        free = [i for i in range(1, amount) if given[i] < largest] or [i for i in range(1, amount) if given[i] < most]
        mass, left = sum([loads[i] for i in free]), spare
        for i in free:
            addition = min(most - given[i], max(1, left * loads[i] // mass), spare)
            given[i] = given[i] + addition
            spare = spare - addition
    return np.array(given)


def gaussian(own_key, dims, width, reach, shards=(), held_as=jnp.bfloat16):
    values = width * jax.random.normal(own_key, dims, jnp.float32)
    if shards:
        values = values * levels(own_key, dims, shards, -0.22, 0.18)
    return jnp.clip(values, -reach, reach).astype(held_as)


def setup_inputs(seed: int = 0) -> dict:
    key_of = jax.random.split(jax.random.key(seed), 18)
    x_in = gaussian(key_of[0], (HEADS * HEAD_DIM, SEQLEN), 1.0, 6.0, ((0, 4), (1, 8)))
    z_in = gaussian(key_of[1], (HEADS * HEAD_DIM, SEQLEN), 1.0, 6.0, ((0, 4), (1, 8)))
    dt_raw = draw_dt_raw(jax.random.fold_in(key_of[17], 71), 0)
    decay_rate = draw_decay_rate(jax.random.fold_in(key_of[17], 71), 0)
    b_in = gaussian(key_of[4], (GROUPS * NSTATE, SEQLEN), 1.0, 6.0, ((1, 8),))
    c_in = gaussian(key_of[5], (GROUPS * NSTATE, SEQLEN), 1.0, 6.0, ((1, 8),))
    conv_x = gaussian(key_of[6], (HEADS * HEAD_DIM, KCONV), KCONV ** -0.5, 3.0, ((0, 4),), jnp.float32)
    conv_b = gaussian(key_of[7], (GROUPS * NSTATE, KCONV), KCONV ** -0.5, 3.0, (), jnp.float32)
    conv_c = gaussian(key_of[8], (GROUPS * NSTATE, KCONV), KCONV ** -0.5, 3.0, (), jnp.float32)
    head_gain = jnp.clip(1.0 + 0.18 * jax.random.normal(key_of[9], (HEADS * HEAD_DIM,), jnp.float32), 0.1, 1.9)
    moe_rows = gaussian(key_of[10], (MTOK, D), 1.0, 6.0, ((0, 8),))
    moe_gain = jnp.clip(1.0 + 0.18 * jax.random.normal(key_of[11], (D,), jnp.float32), 0.1, 1.9)
    routes_keys = jax.random.split(jax.random.fold_in(key_of[12], 1), MTOK // MOE_DEV)
    routes_turns = jax.random.permutation(jax.random.fold_in(key_of[12], 3), MTOK // MOE_DEV)
    routes = jax.vmap(lambda own, number: assign_block(jax.random.fold_in(key_of[12], 2), own, number, MOE_DEV, EXPERTS, TOP, CAP, 2))(routes_keys, routes_turns).reshape((MTOK, TOP))
    route_logit = gaussian(key_of[13], (MTOK, TOP), 1.5, 6.0, ((0, 8),), jnp.float32)
    w_gate = gaussian(key_of[14], (EXPERTS, D, FF), D ** -0.5, 0.125, ((0, 8), (2, 4)))
    w_up = gaussian(key_of[15], (EXPERTS, D, FF), D ** -0.5, 0.125, ((0, 8), (2, 4)))
    w_down = gaussian(key_of[16], (EXPERTS, FF, D), FF ** -0.5, 0.078125, ((0, 8), (1, 4)))
    return dict(x_in=x_in, z_in=z_in, dt_raw=dt_raw, decay_rate=decay_rate, b_in=b_in, c_in=c_in, conv_x=conv_x, conv_b=conv_b, conv_c=conv_c, head_gain=head_gain, moe_rows=moe_rows, moe_gain=moe_gain, routes=routes, route_logit=route_logit, w_gate=w_gate, w_up=w_up, w_down=w_down)


HIGHEST = lax.Precision.HIGHEST
ROW_EPS = 0.1
HEAD_EPS = 1.0

def causal_conv(signal, weight):
    taps = weight.shape[1]
    length = signal.shape[1]
    padded = jnp.pad(signal, ((0, 0), (taps - 1, 0)))
    running = jnp.zeros(signal.shape, jnp.float32)
    for offset in range(taps):
        running = running + weight[:, offset:offset + 1] * padded[:, offset:offset + length]
    return jax.nn.silu(running)

def block_step(state_in, x_block, b_block, c_block, log_block, step_block):
    cum_log = jnp.cumsum(log_block, axis=1)
    seg_log = cum_log[:, :, None] - cum_log[:, None, :]
    causal = jnp.tril(jnp.ones((log_block.shape[1], log_block.shape[1]), bool))
    decay_mask = jnp.exp(jnp.where(causal[None], seg_log, -jnp.inf))
    scores = jnp.einsum('hnt,hns->hts', c_block, b_block, precision=HIGHEST) * decay_mask * step_block[:, None, :]
    inner_term = jnp.einsum('hts,hps->hpt', scores, x_block, precision=HIGHEST)
    carried = jnp.einsum('hnt,hpn->hpt', c_block, state_in, precision=HIGHEST) * jnp.exp(cum_log)[:, None, :]
    tail_weight = jnp.exp(cum_log[:, -1:] - cum_log) * step_block
    fresh_state = jnp.einsum('hps,hns->hpn', x_block * tail_weight[:, None, :], b_block, precision=HIGHEST)
    new_state = jnp.exp(cum_log[:, -1])[:, None, None] * state_in + fresh_state
    return (new_state, inner_term + carried)

def mixer_half(x_in, z_in, dt_raw, decay_rate, b_in, c_in, conv_x, conv_b, conv_c, head_gain):
    x_conv = causal_conv(x_in.astype(jnp.float32), conv_x.astype(jnp.float32)).reshape(HEADS, HEAD_DIM, SEQLEN)
    b_conv = causal_conv(b_in.astype(jnp.float32), conv_b.astype(jnp.float32)).reshape(GROUPS, NSTATE, SEQLEN)
    c_conv = causal_conv(c_in.astype(jnp.float32), conv_c.astype(jnp.float32)).reshape(GROUPS, NSTATE, SEQLEN)
    step_dt = jax.nn.softplus(dt_raw.astype(jnp.float32))
    log_decay = -step_dt * decay_rate.astype(jnp.float32)[:, None]
    block_count = SEQLEN // BLOCK
    per_group = HEADS // GROUPS

    def blocks(tensor):
        return jnp.moveaxis(tensor.reshape(tensor.shape[:-1] + (block_count, BLOCK)), -2, 0)

    def advance(state_in, inputs):
        x_block, b_block, c_block, log_block, step_block = inputs
        return block_step(state_in, x_block, jnp.repeat(b_block, per_group, axis=0), jnp.repeat(c_block, per_group, axis=0), log_block, step_block)
    init_state = jnp.zeros((HEADS, HEAD_DIM, NSTATE), jnp.float32)
    _, block_out = lax.scan(advance, init_state, (blocks(x_conv), blocks(b_conv), blocks(c_conv), blocks(log_decay), blocks(step_dt)))
    y_mixed = jnp.moveaxis(block_out, 0, -2).reshape(HEADS, HEAD_DIM, SEQLEN)
    gated_out = y_mixed * jax.nn.silu(z_in.astype(jnp.float32).reshape(HEADS, HEAD_DIM, SEQLEN))
    head_scale = lax.rsqrt(lax.optimization_barrier(jnp.mean(gated_out * gated_out, axis=1, keepdims=True)) + HEAD_EPS)
    normed_out = gated_out * head_scale * head_gain.astype(jnp.float32).reshape(HEADS, HEAD_DIM, 1)
    return normed_out.reshape(HEADS * HEAD_DIM, SEQLEN).astype(jnp.bfloat16)

def experts_half(moe_rows, moe_gain, routes, route_logit, w_gate, w_up, w_down):
    rows_float = moe_rows.astype(jnp.float32)
    row_scale = lax.rsqrt(lax.optimization_barrier(jnp.mean(rows_float * rows_float, axis=1, keepdims=True)) + ROW_EPS)
    normed = (rows_float * row_scale * moe_gain.astype(jnp.float32)).astype(jnp.bfloat16)
    by_source = routes.reshape(N_EP, MOE_DEV * TOP)
    hit_table = (by_source[:, :, None] == jnp.arange(EXPERTS, dtype=jnp.int32)).astype(jnp.int32)
    slot_rank = lax.optimization_barrier(jnp.sum((jnp.cumsum(hit_table, axis=1) - hit_table) * hit_table, axis=2))
    slot_index = (jnp.arange(N_EP, dtype=jnp.int32)[:, None] * CAP + slot_rank).reshape(-1).astype(jnp.int32)
    expert_index = routes.reshape(-1).astype(jnp.int32)
    token_index = (jnp.arange(MTOK * TOP, dtype=jnp.int32) // TOP).astype(jnp.int32)
    buffer = jnp.zeros((EXPERTS, N_EP * CAP, D), jnp.bfloat16).at[expert_index, slot_index].set(normed[token_index])
    block_width = FF // N_TP

    def run_expert(inputs):
        rows_in, gate_weight, up_weight, down_weight = inputs
        gate_act = jnp.dot(rows_in, gate_weight, preferred_element_type=jnp.float32)
        up_act = jnp.dot(rows_in, up_weight, preferred_element_type=jnp.float32)
        hidden = (jax.nn.silu(gate_act) * up_act).astype(jnp.bfloat16)
        running = jnp.zeros((rows_in.shape[0], D), jnp.float32)
        for part_index in range(N_TP):
            lower = part_index * block_width
            piece_sum = jnp.dot(hidden[:, lower:lower + block_width], down_weight[lower:lower + block_width], preferred_element_type=jnp.float32)
            running = running + lax.optimization_barrier(piece_sum.astype(jnp.bfloat16)).astype(jnp.float32)
        return running.astype(jnp.bfloat16)
    results = lax.map(run_expert, (buffer, w_gate, w_up, w_down))
    picked = results[expert_index, slot_index].astype(jnp.float32).reshape(MTOK, TOP, D)
    weight = jax.nn.sigmoid(route_logit - route_logit[:, ::-1])
    combined = lax.optimization_barrier(jnp.sum(picked * weight[:, :, None], axis=1))
    return combined.T.astype(jnp.bfloat16)

def reference(x_in, z_in, dt_raw, decay_rate, b_in, c_in, conv_x, conv_b, conv_c, head_gain, moe_rows, moe_gain, routes, route_logit, w_gate, w_up, w_down):
    mixed = mixer_half(x_in, z_in, dt_raw, decay_rate, b_in, c_in, conv_x, conv_b, conv_c, head_gain)
    moe_out = experts_half(moe_rows, moe_gain, routes, route_logit, w_gate, w_up, w_down)
    return (mixed, moe_out)
```

```python
import functools

import jax
import jax.numpy as jnp
from jax import lax
from jax.experimental import pallas as pl
from jax.experimental.pallas import tpu as pltpu
from jax.sharding import PartitionSpec as P

HEADS = 64
HEAD_DIM = 64
GROUPS = 2
NSTATE = 128
BLOCK = 128
ROW_EPS = 0.1
HEAD_EPS = 1.0

BF = jnp.bfloat16
F32 = jnp.float32


def sds(shape, dtype):
    return jax.ShapeDtypeStruct(shape, dtype)


def whole(shape):
    return pl.BlockSpec(shape, lambda *a: (0,) * len(shape))


def dot(a, b):
    return jnp.dot(a, b, preferred_element_type=F32)


def silu(v):
    return v * (0.5 + 0.5 * jnp.tanh(0.5 * v))


def call(body, name, ids, ins, outs, grid=(1,), in_specs=None, out_specs=None, scratch=(), flops=0):
    in_specs = in_specs or [whole(a.shape) for a in ins]
    out_specs = out_specs or [whole(o.shape) for o in outs]
    return pl.pallas_call(
        body,
        name=name,
        out_shape=outs,
        grid_spec=pltpu.PrefetchScalarGridSpec(
            num_scalar_prefetch=1,
            grid=grid,
            in_specs=in_specs,
            out_specs=out_specs,
            scratch_shapes=list(scratch),
        ),
        compiler_params=pltpu.CompilerParams(
            dimension_semantics=("arbitrary",) * len(grid), vmem_limit_bytes=60 * 1024 * 1024
        ),
        cost_estimate=pl.CostEstimate(flops=flops, bytes_accessed=0, transcendentals=0)
        if flops
        else None,
    )(ids, *ins)


def ids_of(ids_ref):
    place, column = ids_ref[0], ids_ref[1]
    return place, column // 2, column % 2


def fill_rows(rows, count=8):
    width = rows[0].shape[1]
    at = lax.broadcasted_iota(jnp.int32, (count, width), 0)
    out = jnp.broadcast_to(rows[0], (count, width))
    for index in range(1, len(rows)):
        out = jnp.where(at == index, rows[index], out)
    return out


def destinations(routes_t, place, experts, capacity):
    tokens = routes_t.shape[1]
    relative = jnp.bitwise_xor(routes_t, place)
    first, second = relative[0:1, :], relative[1:2, :]
    at = lax.broadcasted_iota(jnp.int32, (experts, tokens), 0)
    hit_a = (at == first).astype(F32)
    hit_b = (at == second).astype(F32)
    row = lax.broadcasted_iota(jnp.int32, (tokens, tokens), 0)
    col = lax.broadcasted_iota(jnp.int32, (tokens, tokens), 1)
    before = (row < col).astype(F32).astype(BF)
    ahead = dot((hit_a + hit_b).astype(BF), before)
    rank_a = jnp.sum(hit_a * ahead, axis=0, keepdims=True).astype(jnp.int32)
    rank_b = jnp.sum(hit_b * ahead, axis=0, keepdims=True).astype(jnp.int32)
    return first * capacity + rank_a, second * capacity + rank_b


def prep(ids, moe_rows, moe_gain, routes_t, x_in, b_in, c_in, sizes):
    tokens, features = moe_rows.shape
    experts, cap, width, y_count = sizes
    half = experts // 2
    value_rows, length = x_in.shape
    group_rows = b_in.shape[0] // GROUPS

    def body(ids_ref, rows_ref, gain_ref, routes_ref, x_ref, b_ref, c_ref, *refs):
        outs, (normed_ref,) = refs[:-1], refs[-1:]
        self_ref, near, far, rim_ref = outs[0], outs[1:half], outs[half : 2 * half], outs[-1]
        place, y, core = ids_of(ids_ref)
        rows = rows_ref[...].astype(F32)
        scale = lax.rsqrt(jnp.mean(rows * rows, axis=1, keepdims=True) + ROW_EPS)
        normed_ref[...] = (rows * scale * gain_ref[...]).astype(BF)
        dest_a, dest_b = destinations(routes_ref[...], place, experts, cap)

        def pick(index):
            slot = lax.broadcasted_iota(jnp.int32, (cap, tokens), 0) + index * cap
            return ((slot == dest_a) | (slot == dest_b)).astype(F32).astype(BF)

        def columns(block):
            return normed_ref[:, pl.ds(pl.multiple_of(block * width, width), width)]

        mine = columns(2 * y + core)
        for index in range(half):
            far[index][...] = dot(pick(half + index), mine).astype(BF)
        for j in range(y_count):
            part = columns(2 * j + core)
            for index in range(1, half):
                near[index - 1][:, j * width : (j + 1) * width] = dot(pick(index), part).astype(BF)
        self_ref[...] = dot(pick(0), normed_ref[...]).astype(BF)
        group = y * (GROUPS * 2) // (2 * y_count)
        start = pl.multiple_of(group * group_rows, group_rows)
        tail = lax.broadcasted_iota(jnp.int32, (16, 128), 0)
        lane = lax.broadcasted_iota(jnp.int32, (16, 128), 1)
        take = (lane == tail + 125).astype(F32).astype(BF)
        nt = (((1,), (1,)), ((), ()))

        def edge(block):
            return lax.dot_general(take, block, nt, preferred_element_type=F32).astype(BF)

        rim_ref[:, :value_rows] = edge(x_ref[...])
        rim_ref[:, value_rows : value_rows + group_rows] = edge(b_ref[pl.ds(start, group_rows), :])
        rim_ref[:, value_rows + group_rows :] = edge(c_ref[pl.ds(start, group_rows), :])

    last = length // 128 - 1
    outs = [sds((cap, features), BF)]
    outs += [sds((cap, y_count * width), BF)] * (half - 1)
    outs += [sds((cap, width), BF)] * half
    outs += [sds((16, value_rows + 2 * group_rows), BF)]
    return call(
        body,
        "prep",
        ids,
        (moe_rows, moe_gain, routes_t, x_in, b_in, c_in),
        outs,
        in_specs=[
            whole(moe_rows.shape),
            whole(moe_gain.shape),
            whole(routes_t.shape),
            pl.BlockSpec((value_rows, 128), lambda i, s: (0, last)),
            pl.BlockSpec((b_in.shape[0], 128), lambda i, s: (0, last)),
            pl.BlockSpec((c_in.shape[0], 128), lambda i, s: (0, last)),
        ],
        scratch=[pltpu.VMEM((tokens, features), BF)],
    )


def gate_up(ids, self_rows, near, near_other, far, far_other, w_gate, w_up, sizes):
    experts, cap, width, y_count = sizes
    features, hidden = w_gate.shape[1:]
    rows = experts * cap
    split = experts // 2 * cap
    step = 256 if hidden % 256 == 0 else hidden
    pieces = (self_rows, *near, *near_other, *far, *far_other)

    def body(ids_ref, *refs):
        wg_ref, wu_ref, out_ref, lhs_ref = refs[len(pieces) :]
        self_ref = refs[0]
        at = 1
        near_ref = refs[at : at + len(near)]
        at += len(near)
        near_o_ref = refs[at : at + len(near_other)]
        at += len(near_other)
        far_ref = refs[at : at + len(far)]
        at += len(far)
        far_o_ref = refs[at : at + len(far_other)]
        _, y, core = ids_of(ids_ref)

        def columns(block):
            return pl.ds(pl.multiple_of(block * width, width), width)

        @pl.when(pl.program_id(0) == 0)
        def _():
            lhs_ref[0:cap, :] = self_ref[...]
            for source, c in ((near_ref, core), (near_o_ref, 1 - core)):
                for ref in source:
                    for j in range(y_count):
                        lhs_ref[cap:split, columns(2 * j + c)] = ref[:, j * width : (j + 1) * width]
            for source, c in ((far_ref, core), (far_o_ref, 1 - core)):
                for j, ref in enumerate(source):
                    lhs_ref[split:rows, columns(2 * jnp.bitwise_xor(y, j) + c)] = ref[...]

        lhs = lhs_ref[...]
        gate = dot(lhs, wg_ref[0])
        up = dot(lhs, wu_ref[0])
        out_ref[...] = (silu(gate) * up).astype(BF)

    return call(
        body,
        "gate_up",
        ids,
        (*pieces, w_gate, w_up),
        [sds((rows, hidden), BF)],
        grid=(hidden // step,),
        in_specs=[whole(a.shape) for a in pieces]
        + [pl.BlockSpec((1, features, step), lambda i, s: (0, 0, i))] * 2,
        out_specs=[pl.BlockSpec((rows, step), lambda i, s: (0, i))],
        scratch=[pltpu.VMEM((rows, features), BF)],
        flops=4 * rows * features * hidden,
    )[0]


def down(ids, hidden, w_down, sizes, flip):
    experts, cap, width, y_count = sizes
    rows, depth = hidden.shape

    def body(ids_ref, h_ref, w_ref, out_ref):
        out_ref[...] = dot(h_ref[...], w_ref[0]).astype(BF)

    def block(i, s):
        core = s[1] % 2
        return (0, 0, 2 * i + (1 - core if flip else core))

    return call(
        body,
        "down_send" if flip else "down_keep",
        ids,
        (hidden, w_down),
        [sds((rows, y_count * width), BF)],
        grid=(y_count,),
        in_specs=[whole(hidden.shape), pl.BlockSpec((1, depth, width), block)],
        out_specs=[pl.BlockSpec((rows, width), lambda i, s: (0, i))],
        flops=2 * rows * depth * y_count * width,
    )[0]


def core_sum(ids, keep, received, sizes):
    experts, cap, width, y_count = sizes
    half = experts // 2
    split = half * cap
    rows = experts * cap

    def body(ids_ref, keep_ref, recv_ref, *outs):
        _, y, _ = ids_of(ids_ref)
        near, far_keep, far_send = outs[:half], outs[half], outs[half + 1 :]
        for index in range(half):
            span = pl.ds(index * cap, cap)
            near[index][...] = (
                keep_ref[span, :].astype(F32) + recv_ref[span, :].astype(F32)
            ).astype(BF)
        for j in range(y_count):
            column = pl.ds(pl.multiple_of(jnp.bitwise_xor(y, j) * width, width), width)
            total = keep_ref[split:rows, column].astype(F32) + recv_ref[split:rows, column].astype(F32)
            target = far_keep if j == 0 else far_send[j - 1]
            target[...] = total.astype(BF)

    outs = [sds((cap, y_count * width), BF)] * half + [sds((split, width), BF)] * y_count
    return call(body, "core_sum", ids, (keep, received), outs)


def far_sum(ids, parts, sizes):
    experts, cap, width, y_count = sizes
    half = experts // 2

    def body(ids_ref, *refs):
        ins, outs = refs[: len(parts)], refs[len(parts) :]
        for index in range(half):
            span = pl.ds(index * cap, cap)
            total = ins[0][span, :].astype(F32)
            for ref in ins[1:]:
                total = total + ref[span, :].astype(F32)
            outs[index][...] = total.astype(BF)

    return call(body, "far_sum", ids, parts, [sds((cap, width), BF)] * half)


def token_weights(place, routes_t, logit_t, experts, cap):
    tokens = routes_t.shape[1]
    dest_a, dest_b = destinations(routes_t, place, experts, cap)
    gap = logit_t[0:1, :] - logit_t[1:2, :]
    weight_a, weight_b = jax.nn.sigmoid(gap), jax.nn.sigmoid(-gap)
    table = fill_rows([dest_a.astype(F32), dest_b.astype(F32), weight_a, weight_b]).T
    first, second = table[:, 0:1], table[:, 1:2]
    share_a, share_b = table[:, 2:3], table[:, 3:4]

    def pick(index):
        slot = (lax.broadcasted_iota(jnp.int32, (tokens, cap), 1) + index * cap).astype(F32)
        return (
            jnp.where(slot == first, share_a, 0.0) + jnp.where(slot == second, share_b, 0.0)
        ).astype(BF)

    return pick


def near_combine(ids, parts, routes_t, logit_t, sizes):
    experts, cap, width, y_count = sizes
    tokens = routes_t.shape[1]

    def body(ids_ref, routes_ref, logit_ref, *refs):
        ins, outs = refs[: len(parts)], refs[len(parts) :]
        place, y, _ = ids_of(ids_ref)
        pick = token_weights(place, routes_ref[...], logit_ref[...], experts, cap)
        picks = [pick(index) for index in range(len(parts))]
        for j in range(y_count):
            column = pl.ds(pl.multiple_of(jnp.bitwise_xor(y, j) * width, width), width)
            total = dot(picks[0], ins[0][:, column])
            for index in range(1, len(parts)):
                total = total + dot(picks[index], ins[index][:, column])
            outs[j][...] = total.astype(outs[j].dtype)

    outs = [sds((tokens, width), F32)] + [sds((tokens, width), BF)] * (y_count - 1)
    return call(body, "near_combine", ids, (routes_t, logit_t, *parts), outs)


def final_combine(ids, parts, near_keep, near_received, routes_t, logit_t, sizes):
    experts, cap, width, y_count = sizes
    tokens = routes_t.shape[1]
    half = experts // 2

    def body(ids_ref, routes_ref, logit_ref, keep_ref, *refs):
        received, ins, out_ref = refs[: y_count - 1], refs[y_count - 1 : -1], refs[-1]
        place, _, _ = ids_of(ids_ref)
        pick = token_weights(place, routes_ref[...], logit_ref[...], experts, cap)
        total = keep_ref[...]
        for ref in received:
            total = total + ref[...].astype(F32)
        for index in range(half):
            total = total + dot(pick(half + index), ins[index][...])
        out_ref[...] = total.astype(BF)

    return call(
        body,
        "final_combine",
        ids,
        (routes_t, logit_t, near_keep, *near_received, *parts),
        [sds((tokens, width), BF)],
    )[0]


def swap(value, axis, step):
    count = lax.axis_size(axis)
    return lax.ppermute(value, axis, [(i, i ^ step) for i in range(count)])


def tall(rows):
    return jnp.transpose(fill_rows(rows))


def conv_block(signal, rim_t, taps_t):
    rows, length = signal.shape
    kinds = [taps_t[k : k + 1, :] for k in range(taps_t.shape[0])]
    taps = tall(kinds)
    count = len(kinds)
    place = lax.broadcasted_iota(jnp.int32, (16, 128), 0)
    lane = lax.broadcasted_iota(jnp.int32, (16, 128), 1)
    put = ((lane == place + 125) & (place < 3)).astype(F32).astype(BF)
    edge = dot(jnp.transpose(rim_t.astype(F32)).astype(BF), put)
    value = signal.astype(F32)
    joined = jnp.concatenate([edge, value], axis=1)
    total = taps[:, count - 1 : count] * value
    for back in range(1, count):
        total = total + taps[:, count - 1 - back : count - back] * pltpu.roll(joined, back, 1)[:, 128:]
    return silu(total)


def head_rows(table, heads_here, length):
    return jnp.concatenate(
        [jnp.broadcast_to(table[i : i + 1, :], (HEAD_DIM, length)) for i in range(heads_here)], axis=0
    )


def mixer_open(ids, x_in, dt_raw, rate_row, b_in, c_in, taps_x, taps_b, taps_c, rims, hb, hp, y_count):
    rows, length = x_in.shape
    heads = dt_raw.shape[0]
    block_rows = hb * HEAD_DIM

    def body(ids_ref, x_ref, dt_ref, rate_ref, b_ref, c_ref, tx_ref, tb_ref, tc_ref, rx_ref, rbc_ref, *outs):
        xs_ref, cum_ref, bt_ref, conv_c_ref, msg_ref, step_ref = outs
        _, y, _ = ids_of(ids_ref)
        turn = pl.program_id(0)

        @pl.when(turn == 0)
        def _():
            group = y * (GROUPS * 2) // (2 * y_count)
            start = pl.multiple_of(group * NSTATE, NSTATE)
            span = pl.ds(start, NSTATE)
            b_conv = conv_block(b_ref[span, :], rbc_ref[:, :NSTATE], tb_ref[:, span])
            c_conv = conv_block(c_ref[span, :], rbc_ref[:, NSTATE:], tc_ref[:, span])
            bt_ref[...] = jnp.transpose(b_conv).astype(BF)
            conv_c_ref[...] = c_conv.astype(BF)
            raw = dt_ref[...]
            step = jnp.maximum(raw, 0.0) + jnp.log1p(jnp.exp(-jnp.abs(raw)))
            eye_r = lax.broadcasted_iota(jnp.int32, (heads, heads), 0)
            eye_c = lax.broadcasted_iota(jnp.int32, (heads, heads), 1)
            rate = jnp.sum(jnp.where(eye_r == eye_c, rate_ref[...], 0.0), axis=1, keepdims=True)
            cum = -step * rate
            lane = lax.broadcasted_iota(jnp.int32, (heads, length), 1)
            shift = 1
            while shift < length:
                cum = cum + jnp.where(lane >= shift, pltpu.roll(cum, shift, 1), 0.0)
                shift *= 2
            step_ref[...] = step
            cum_ref[...] = cum
            total = jnp.broadcast_to(jnp.exp(cum[:, length - 1 : length]), (heads, NSTATE))
            if heads < hp:
                total = jnp.concatenate([total, jnp.ones((hp - heads, NSTATE), F32)], axis=0)
            high = total.astype(BF)
            msg_ref[rows : rows + hp, :] = high
            msg_ref[rows + hp : rows + 2 * hp, :] = (total - high.astype(F32)).astype(BF)

        value = conv_block(x_ref[...], rx_ref[...], tx_ref[...])
        first = turn * hb if heads > hb else 0
        step = step_ref[pl.ds(first, hb), :]
        cum = cum_ref[pl.ds(first, hb), :]
        fade = jnp.exp(cum[:, length - 1 : length] - cum)
        scaled = value * head_rows(step, hb, length)
        xs_ref[...] = scaled.astype(BF)
        state = dot((scaled * head_rows(fade, hb, length)).astype(BF), bt_ref[...])
        msg_ref[pl.ds(pl.multiple_of(turn * block_rows, block_rows), block_rows), :] = state.astype(BF)

    outs = [
        sds((rows, length), BF),
        sds((heads, length), F32),
        sds((length, NSTATE), BF),
        sds((NSTATE, length), BF),
        sds((rows + 2 * hp, NSTATE), BF),
    ]
    return call(
        body,
        "mixer_open",
        ids,
        (x_in, dt_raw, rate_row, b_in, c_in, taps_x, taps_b, taps_c, rims[:, :rows], rims[:, rows:]),
        outs,
        grid=(heads // hb,),
        in_specs=[
            pl.BlockSpec((block_rows, length), lambda i, s: (i, 0)),
            whole(dt_raw.shape),
            whole(rate_row.shape),
            whole(b_in.shape),
            whole(c_in.shape),
            pl.BlockSpec((taps_x.shape[0], block_rows), lambda i, s: (0, i)),
            whole(taps_b.shape),
            whole(taps_c.shape),
            pl.BlockSpec((16, block_rows), lambda i, s: (0, i)),
            whole((16, 2 * NSTATE)),
        ],
        out_specs=[pl.BlockSpec((block_rows, length), lambda i, s: (i, 0))]
        + [whole(o.shape) for o in outs[1:]],
        scratch=[pltpu.VMEM((heads, length), F32)],
    )


def per_row(table, heads, hp):
    width = table.shape[1]
    return jnp.broadcast_to(table[:heads][:, None, :], (heads, HEAD_DIM, width)).reshape(
        heads * HEAD_DIM, width
    )


def state_round(ids, mine, received, carried, level, heads, hp):
    rows = heads * HEAD_DIM
    opening = carried is None
    outs = [sds(mine.shape, BF), sds((rows, NSTATE), F32), sds((hp, NSTATE), F32)]

    def body(ids_ref, mine_ref, recv_ref, *refs):
        msg_ref, pre_ref, dec_ref = refs[-3:]
        upper = (ids_ref[0] >> level) % 2 == 1
        t_mine = mine_ref[:rows, :].astype(F32)
        t_recv = recv_ref[:rows, :].astype(F32)

        def decay(ref):
            return ref[rows : rows + hp, :].astype(F32) + ref[rows + hp :, :].astype(F32)

        d_mine, d_recv = decay(mine_ref), decay(recv_ref)
        one = jnp.ones_like(d_mine)
        d_late = jnp.where(upper, d_mine, d_recv)
        late = jnp.where(upper, t_mine, t_recv)
        early = jnp.where(upper, t_recv, t_mine)
        total = late + per_row(d_late, heads, hp) * early
        msg_ref[:rows, :] = total.astype(BF)
        both = d_mine * d_recv
        high = both.astype(BF)
        msg_ref[rows : rows + hp, :] = high
        msg_ref[rows + hp :, :] = (both - high.astype(F32)).astype(BF)
        if opening:
            pre_ref[...] = jnp.where(upper, t_recv, jnp.zeros_like(t_recv))
            dec_ref[...] = jnp.where(upper, d_recv, one)
        else:
            old_pre, old_dec = refs[0], refs[1]
            grown = old_pre[...] + per_row(old_dec[...], heads, hp) * t_recv
            pre_ref[...] = jnp.where(upper, grown, old_pre[...])
            dec_ref[...] = jnp.where(upper, old_dec[...] * d_recv, old_dec[...])

    ins = (mine, received) if opening else (mine, received, *carried)
    return call(body, "state_round", ids, ins, outs)


def mixer_close(ids, carried, received, xs, cum, b_t, c_conv, z_in, gain_row, hb, hp):
    rows, length = xs.shape
    heads = cum.shape[0]
    block_rows = hb * HEAD_DIM
    blocks = length // BLOCK

    def body(ids_ref, pre_ref, dec_ref, recv_ref, xs_ref, cum_ref, bt_ref, c_ref, z_ref, gain_ref, out_ref, gram_ref, y_ref):
        turn = pl.program_id(0)

        @pl.when(turn == 0)
        def _():
            row = lax.broadcasted_iota(jnp.int32, (BLOCK, BLOCK), 0)
            col = lax.broadcasted_iota(jnp.int32, (BLOCK, BLOCK), 1)
            for j in range(blocks):
                span = slice(j * BLOCK, (j + 1) * BLOCK)
                gram = dot(bt_ref[span, :], c_ref[:, span])
                gram_ref[j] = jnp.where(row <= col, gram, 0.0)

        first = turn * hb if heads > hb else 0
        decay = dec_ref[pl.ds(first, hb), :]
        state = pre_ref[...] + head_rows(decay, hb, NSTATE) * recv_ref[...].astype(F32)
        cum = cum_ref[...]
        down_cum = jnp.transpose(fill_rows([cum[i : i + 1, :] for i in range(hb)]))
        before = jnp.zeros((hb, 1), F32)
        for j in range(blocks):
            span = slice(j * BLOCK, (j + 1) * BLOCK)
            here = cum[:, span]
            after = here[:, BLOCK - 1 : BLOCK]
            c_block = c_ref[:, span]
            flow = dot(state.astype(BF), c_block) * head_rows(jnp.exp(here - before), hb, BLOCK)
            gram = gram_ref[j]
            for i in range(hb):
                lines = slice(i * HEAD_DIM, (i + 1) * HEAD_DIM)
                gap = jnp.minimum(here[i : i + 1, :] - down_cum[span, i : i + 1], 0.0)
                mask = (gram * jnp.exp(gap)).astype(BF)
                y_ref[lines, span] = flow[lines, :] + dot(xs_ref[lines, span], mask)
            if j + 1 < blocks:
                fade = head_rows(jnp.exp(after - here), hb, BLOCK)
                fresh = dot((xs_ref[:, span].astype(F32) * fade).astype(BF), bt_ref[span, :])
                kept = head_rows(jnp.broadcast_to(jnp.exp(after - before), (hb, NSTATE)), hb, NSTATE)
                state = kept * state + fresh
            before = after
        gain = tall([gain_ref[...]])
        for i in range(hb):
            lines = slice(i * HEAD_DIM, (i + 1) * HEAD_DIM)
            gated = y_ref[lines, :] * silu(z_ref[lines, :].astype(F32))
            scale = lax.rsqrt(jnp.mean(gated * gated, axis=0, keepdims=True) + HEAD_EPS)
            out_ref[lines, :] = (gated * scale * gain[lines, 0:1]).astype(BF)

    pre, dec = carried
    tile = pl.BlockSpec((block_rows, length), lambda i, s: (i, 0))
    state_tile = pl.BlockSpec((block_rows, NSTATE), lambda i, s: (i, 0))
    return call(
        body,
        "mixer_close",
        ids,
        (pre, dec, received, xs, cum, b_t, c_conv, z_in, gain_row),
        [sds((rows, length), BF)],
        grid=(heads // hb,),
        in_specs=[
            state_tile,
            whole(dec.shape),
            state_tile,
            tile,
            pl.BlockSpec((hb, length), lambda i, s: (i, 0)),
            whole(b_t.shape),
            whole(c_conv.shape),
            tile,
            pl.BlockSpec((1, block_rows), lambda i, s: (0, i)),
        ],
        out_specs=[tile],
        scratch=[pltpu.VMEM((blocks, BLOCK, BLOCK), F32), pltpu.VMEM((block_rows, length), F32)],
    )[0]


def on_device(
    x_in,
    z_in,
    dt_raw,
    decay_rate,
    b_in,
    c_in,
    conv_x,
    conv_b,
    conv_c,
    head_gain,
    moe_rows,
    moe_gain,
    routes,
    route_logit,
    w_gate,
    w_up,
    w_down,
):
    ep, tp = lax.axis_size("ep"), lax.axis_size("tp")
    y_count = tp // 2
    heads = dt_raw.shape[0]
    hb, hp = min(8, heads), -(-heads // 16) * 16
    tokens, features = moe_rows.shape
    experts = ep * w_gate.shape[0]
    capacity = 2 * tokens * routes.shape[1] // experts
    cap = -(-capacity // 16) * 16
    sizes = (experts, cap, features // tp, y_count)
    half = experts // 2
    ids = jnp.stack([lax.axis_index("ep"), lax.axis_index("tp")]).astype(jnp.int32)
    routes_t, logit_t = routes.T, route_logit.T

    outs = prep(ids, moe_rows, moe_gain.reshape(1, -1), routes_t, x_in, b_in, c_in, sizes)
    self_rows, near, far, own_rims = outs[0], outs[1:half], outs[half : 2 * half], outs[-1]
    rims = lax.ppermute(own_rims, "ep", [(i, i + 1) for i in range(ep - 1)])
    far = [swap(value, "ep", half + index) for index, value in enumerate(far)]
    near = [swap(value, "ep", 1 + index) for index, value in enumerate(near)]
    far_all = jnp.concatenate(far, axis=0)
    far_all = [far_all] + [swap(far_all, "tp", 2 * j) for j in range(1, y_count)]
    near_all = [jnp.concatenate(near, axis=0)]
    near_other = [swap(value, "tp", 1) for value in near_all]
    far_other = [swap(value, "tp", 1) for value in far_all]

    xs, cum, b_t, c_conv, message = mixer_open(
        ids,
        x_in,
        dt_raw,
        decay_rate.reshape(1, -1),
        b_in,
        c_in,
        conv_x.T,
        conv_b.T,
        conv_c.T,
        rims,
        hb,
        hp,
        y_count,
    )
    carried, level = None, 0
    while (2 << level) < ep:
        received = swap(message, "ep", 1 << level)
        message, *carried = state_round(ids, message, received, carried, level, heads, hp)
        level += 1
    top = 1 << level
    last = lax.ppermute(message, "ep", [(i, i + top) for i in range(ep - top)])

    hidden = gate_up(ids, self_rows, near_all, near_other, far_all, far_other, w_gate, w_up, sizes)
    send = down(ids, hidden, w_down, sizes, True)
    received = swap(send, "tp", 1)
    keep = down(ids, hidden, w_down, sizes, False)
    outs = core_sum(ids, keep, received, sizes)
    near_out, far_keep, far_send = outs[:half], outs[half], outs[half + 1 :]
    far_parts = [far_keep] + [swap(value, "tp", 2 * (j + 1)) for j, value in enumerate(far_send)]
    near_back = [near_out[0]] + [swap(near_out[k], "ep", k) for k in range(1, half)]
    far_out = far_sum(ids, far_parts, sizes)
    far_back = [swap(value, "ep", half + index) for index, value in enumerate(far_out)]
    outs = near_combine(ids, near_back, routes_t, logit_t, sizes)
    near_keep = outs[0]
    near_received = [swap(value, "tp", 2 * (j + 1)) for j, value in enumerate(outs[1:])]
    moe_t = final_combine(ids, far_back, near_keep, near_received, routes_t, logit_t, sizes)

    mixed = mixer_close(
        ids, carried, last, xs, cum, b_t, c_conv, z_in, head_gain.reshape(1, -1), hb, hp
    )
    return (mixed, moe_t.T)


def solution(mesh):
    return jax.shard_map(
        on_device,
        mesh=mesh,
        in_specs=(
            P("tp", "ep"),
            P("tp", "ep"),
            P("tp", "ep"),
            P("tp"),
            P(None, "ep"),
            P(None, "ep"),
            P("tp", None),
            P(),
            P(),
            P("tp"),
            P("ep", None),
            P(),
            P("ep", None),
            P("ep", None),
            P("ep", None, "tp"),
            P("ep", None, "tp"),
            P("ep", "tp", None),
        ),
        out_specs=(P("tp", "ep"), P("tp", "ep")),
        check_vma=False,
    )
```

```python
import jax
import jax.numpy as jnp
from jax import lax
from jax.experimental import pallas as pl
from jax.experimental.pallas import tpu as pltpu
from jax.sharding import PartitionSpec as P


HEAD_DIM = 64
GROUPS = 2
NSTATE = 128
BLOCK = 128
ROW_EPS = 0.1
HEAD_EPS = 1.0

BF = jnp.bfloat16
F32 = jnp.float32


def sds(shape, dtype):
    return jax.ShapeDtypeStruct(shape, dtype)


def whole(shape):
    return pl.BlockSpec(shape, lambda *a: (0,) * len(shape))


def dot(a, b):
    return jnp.dot(a, b, preferred_element_type=F32)


def silu(v):
    return v * (0.5 + 0.5 * jnp.tanh(0.5 * v))


def call(body, name, ids, *args, **kwargs):
    return launch(body, name, ids, *args, **kwargs)


def launch(body, name, ids, ins, outs, grid=None, in_specs=None, out_specs=None, scratch=(), us=1.0, mib=6):
    vmem = pl.BlockSpec(memory_space=pltpu.VMEM)
    common = dict(
        name=name,
        out_shape=outs,
        cost_estimate=pl.CostEstimate(
            flops=int(us * 2.5e8), bytes_accessed=0, transcendentals=0
        ),
    )
    limit = mib * 1024 * 1024
    if grid is None:
        return pl.pallas_call(
            body,
            in_specs=[pl.BlockSpec(memory_space=pltpu.SMEM)] + (in_specs or [vmem] * len(ins)),
            out_specs=out_specs or [vmem] * len(outs),
            scratch_shapes=list(scratch),
            compiler_params=pltpu.CompilerParams(vmem_limit_bytes=limit),
            **common,
        )(ids, *ins)
    return pl.pallas_call(
        body,
        grid_spec=pltpu.PrefetchScalarGridSpec(
            num_scalar_prefetch=1,
            grid=grid,
            in_specs=in_specs,
            out_specs=out_specs,
            scratch_shapes=list(scratch),
        ),
        compiler_params=pltpu.CompilerParams(
            dimension_semantics=("arbitrary",) * len(grid), vmem_limit_bytes=limit
        ),
        **common,
    )(ids, *ins)


GATE_MIB = 24
DOWN_MIB = 16
OPEN_MIB = 28


def in_hbm(value):
    return pltpu.with_memory_space_constraint(value, pltpu.HBM)


def ids_of(ids_ref):
    place, column = ids_ref[0], ids_ref[1]
    return place, column // 2, column % 2


def fill_rows(rows, count=8):
    width = rows[0].shape[1]
    at = lax.broadcasted_iota(jnp.int32, (count, width), 0)
    out = jnp.broadcast_to(rows[0], (count, width))
    for index in range(1, len(rows)):
        out = jnp.where(at == index, rows[index], out)
    return out


def destinations(routes_t, place, experts, capacity):
    tokens = routes_t.shape[1]
    relative = jnp.bitwise_xor(routes_t, place)
    first, second = relative[0:1, :], relative[1:2, :]
    at = lax.broadcasted_iota(jnp.int32, (experts, tokens), 0)
    hit_a = (at == first).astype(F32)
    hit_b = (at == second).astype(F32)
    row = lax.broadcasted_iota(jnp.int32, (tokens, tokens), 0)
    col = lax.broadcasted_iota(jnp.int32, (tokens, tokens), 1)
    before = (row < col).astype(F32).astype(BF)
    ahead = dot((hit_a + hit_b).astype(BF), before)
    rank_a = jnp.sum(hit_a * ahead, axis=0, keepdims=True).astype(jnp.int32)
    rank_b = jnp.sum(hit_b * ahead, axis=0, keepdims=True).astype(jnp.int32)
    return first * capacity + rank_a, second * capacity + rank_b


def prep(ids, moe_rows, moe_gain, routes_t, logit_t, x_in, b_in, c_in, sizes):
    tokens, features = moe_rows.shape
    experts, cap, width, y_count = sizes
    half = experts // 2
    value_rows, length = x_in.shape
    group_rows = b_in.shape[0] // GROUPS

    def body(ids_ref, rows_hbm, gain_hbm, routes_hbm, logit_hbm, x_hbm, b_hbm, c_hbm, *refs):
        outs, scratch = refs[:-9], refs[-9:]
        normed_ref, sems = scratch[0], scratch[-1]
        rows_ref, gain_ref, routes_ref, logit_ref, x_ref, b_ref, c_ref = scratch[1:-1]
        self_ref, near, far = outs[0], outs[1:half], outs[half : 2 * half]
        table_ref, rim_ref = outs[-2:]
        place, y, core = ids_of(ids_ref)
        tail = (slice(None), slice(length - 128, length))
        moves = (
            (rows_hbm, rows_ref),
            (gain_hbm, gain_ref),
            (routes_hbm, routes_ref),
            (logit_hbm, logit_ref),
            (x_hbm.at[tail], x_ref),
            (b_hbm.at[tail], b_ref),
            (c_hbm.at[tail], c_ref),
        )
        copies = [
            pltpu.make_async_copy(source, target, sems.at[index])
            for index, (source, target) in enumerate(moves)
        ]
        for copy in copies:
            copy.start()
        for copy in copies:
            copy.wait()
        rows = rows_ref[...].astype(F32)
        scale = lax.rsqrt(jnp.mean(rows * rows, axis=1, keepdims=True) + ROW_EPS)
        normed_ref[...] = (rows * scale * gain_ref[...]).astype(BF)
        dest_a, dest_b = destinations(routes_ref[...], place, experts, cap)

        def pick(index):
            slot = lax.broadcasted_iota(jnp.int32, (cap, tokens), 0) + index * cap
            return ((slot == dest_a) | (slot == dest_b)).astype(F32).astype(BF)

        def columns(block):
            return normed_ref[:, pl.ds(pl.multiple_of(block * width, width), width)]

        mine = columns(2 * y + core)
        for index in range(half):
            far[index][...] = dot(pick(half + index), mine).astype(BF)
        for j in range(y_count):
            part = columns(2 * j + core)
            for index in range(1, half):
                near[index - 1][:, j * width : (j + 1) * width] = dot(pick(index), part).astype(BF)
        self_ref[...] = dot(pick(0), normed_ref[...]).astype(BF)
        gap = logit_ref[0:1, :] - logit_ref[1:2, :]
        shares = [jax.nn.sigmoid(gap), jax.nn.sigmoid(-gap)]
        table_ref[...] = jnp.transpose(
            fill_rows([dest_a.astype(F32), dest_b.astype(F32)] + shares)
        )
        group = y * (GROUPS * 2) // (2 * y_count)
        start = pl.multiple_of(group * group_rows, group_rows)
        tail = lax.broadcasted_iota(jnp.int32, (16, 128), 0)
        lane = lax.broadcasted_iota(jnp.int32, (16, 128), 1)
        take = (lane == tail + 125).astype(F32).astype(BF)
        nt = (((1,), (1,)), ((), ()))

        def edge(block):
            return lax.dot_general(take, block, nt, preferred_element_type=F32).astype(BF)

        rim_ref[:, :value_rows] = edge(x_ref[...])
        rim_ref[:, value_rows : value_rows + group_rows] = edge(b_ref[pl.ds(start, group_rows), :])
        rim_ref[:, value_rows + group_rows :] = edge(c_ref[pl.ds(start, group_rows), :])

    outs = [sds((cap, features), BF)]
    outs += [sds((cap, y_count * width), BF)] * (half - 1)
    outs += [sds((cap, width), BF)] * half
    outs += [sds((tokens, 8), F32), sds((16, value_rows + 2 * group_rows), BF)]
    return call(
        body,
        "prep",
        ids,
        tuple(map(in_hbm, (moe_rows, moe_gain, routes_t, logit_t, x_in, b_in, c_in))),
        outs,
        in_specs=[pl.BlockSpec(memory_space=pltpu.HBM)] * 7,
        scratch=[
            pltpu.VMEM((tokens, features), BF),
            pltpu.VMEM(moe_rows.shape, BF),
            pltpu.VMEM(moe_gain.shape, F32),
            pltpu.VMEM(routes_t.shape, jnp.int32),
            pltpu.VMEM(logit_t.shape, F32),
            pltpu.VMEM((value_rows, 128), BF),
            pltpu.VMEM((b_in.shape[0], 128), BF),
            pltpu.VMEM((c_in.shape[0], 128), BF),
            pltpu.SemaphoreType.DMA((7,)),
        ],
        us=3.0,
        mib=10,
    )


def gate_up(ids, self_rows, near, near_other, far, far_other, w_gate, w_up, w_down, sizes):
    experts, cap, width, y_count = sizes
    features, hidden = w_gate.shape[1:]
    rows = experts * cap
    split = experts // 2 * cap
    step = 256 if hidden % 256 == 0 else hidden
    groups = (near, near_other, *far, *far_other)
    pieces = (self_rows, *(value for group in groups for value in group))

    def body(ids_ref, *refs):
        wg_ref, wu_ref, wd_ref, low_ref, high_ref, held_ref, lhs_ref, sem = refs[len(pieces) :]
        copy = pltpu.make_async_copy(wd_ref, held_ref, sem)
        copy.start()
        at, held = 1, []
        for group in groups:
            held.append(refs[at : at + len(group)])
            at += len(group)
        _, y, core = ids_of(ids_ref)

        def columns(block):
            return pl.ds(pl.multiple_of(block * width, width), width)

        lhs_ref[0:cap, :] = refs[0][...]
        for source, c in ((held[0], core), (held[1], 1 - core)):
            for index, ref in enumerate(source):
                lines = slice(cap * (1 + index), cap * (2 + index))
                for j in range(y_count):
                    lhs_ref[lines, columns(2 * j + c)] = ref[:, j * width : (j + 1) * width]
        for set_at, c in ((2, core), (2 + len(far), 1 - core)):
            start = split
            for source in held[set_at : set_at + len(far)]:
                tall_rows = source[0].shape[0]
                for j, ref in enumerate(source):
                    lines = slice(start, start + tall_rows)
                    lhs_ref[lines, columns(2 * jnp.bitwise_xor(y, j) + c)] = ref[...]
                start += tall_rows

        for turn in range(hidden // step):
            span = slice(turn * step, (turn + 1) * step)
            for lines, out_ref in ((slice(0, split), low_ref), (slice(split, rows), high_ref)):
                lhs = lhs_ref[lines, :]
                gate = dot(lhs, wg_ref[0, :, span])
                up = dot(lhs, wu_ref[0, :, span])
                out_ref[:, span] = (silu(gate) * up).astype(BF)
        copy.wait()

    vmem = pl.BlockSpec(memory_space=pltpu.VMEM)
    return call(
        body,
        "gate_up",
        ids,
        (*pieces, w_gate, w_up, in_hbm(w_down)),
        [sds((split, hidden), BF)] * 2 + [sds(w_down.shape, w_down.dtype)],
        in_specs=[vmem] * (len(pieces) + 2) + [pl.BlockSpec(memory_space=pltpu.HBM)],
        scratch=[pltpu.VMEM((rows, features), BF), pltpu.SemaphoreType.DMA],
        us=9.0,
        mib=GATE_MIB,
    )


def down(ids, hidden, w_down, sizes, name):
    _, _, width, y_count = sizes
    rows, _ = hidden.shape

    def body(ids_ref, h_ref, w_ref, send_ref, keep_ref):
        core = ids_ref[1] % 2
        for out_ref, c in ((send_ref, 1 - core), (keep_ref, core)):
            for j in range(y_count):
                column = pl.ds(pl.multiple_of((2 * j + c) * width, width), width)
                value = dot(h_ref[...], w_ref[0, :, column])
                out_ref[:, j * width : (j + 1) * width] = value.astype(BF)

    return call(
        body,
        name,
        ids,
        (hidden, w_down),
        [sds((rows, y_count * width), BF)] * 2,
        us=2.0,
        mib=DOWN_MIB,
    )


def near_sum(ids, keep, received, sizes):
    experts, cap, width, y_count = sizes
    half = experts // 2

    def body(ids_ref, keep_ref, recv_ref, *outs):
        for index in range(half):
            span = pl.ds(index * cap, cap)
            outs[index][...] = (
                keep_ref[span, :].astype(F32) + recv_ref[span, :].astype(F32)
            ).astype(BF)

    outs = [sds((cap, y_count * width), BF)] * half
    return call(body, "near_sum", ids, (keep, received), outs)


def far_split(ids, keep, received, sizes):
    _, _, width, y_count = sizes
    rows = keep.shape[0]

    def body(ids_ref, keep_ref, recv_ref, *outs):
        _, y, _ = ids_of(ids_ref)
        for part in range(2):
            lines = pl.ds(part * rows // 2, rows // 2)
            for j in range(y_count):
                column = pl.ds(pl.multiple_of(jnp.bitwise_xor(y, j) * width, width), width)
                outs[part * y_count + j][...] = (
                    keep_ref[lines, column].astype(F32) + recv_ref[lines, column].astype(F32)
                ).astype(BF)

    outs = [sds((rows // 2, width), BF)] * (2 * y_count)
    return call(body, "far_split", ids, (keep, received), outs)


def far_sum(ids, parts, sizes, name):
    experts, cap, width, _ = sizes
    count = experts // 4

    def body(ids_ref, *refs):
        ins, outs = refs[: len(parts)], refs[len(parts) :]
        for index in range(count):
            span = pl.ds(index * cap, cap)
            total = ins[0][span, :].astype(F32)
            for ref in ins[1:]:
                total = total + ref[span, :].astype(F32)
            outs[index][...] = total.astype(BF)

    return call(body, name, ids, parts, [sds((cap, width), BF)] * count)


def token_weights(table, cap):
    tokens = table.shape[0]
    first, second = table[:, 0:1], table[:, 1:2]
    share_a, share_b = table[:, 2:3], table[:, 3:4]

    def pick(index):
        slot = (lax.broadcasted_iota(jnp.int32, (tokens, cap), 1) + index * cap).astype(F32)
        return (
            jnp.where(slot == first, share_a, 0.0) + jnp.where(slot == second, share_b, 0.0)
        ).astype(BF)

    return pick


def near_combine(ids, parts, table, sizes):
    _, cap, width, y_count = sizes
    tokens = table.shape[0]

    def body(ids_ref, table_ref, *refs):
        ins, outs = refs[: len(parts)], refs[len(parts) :]
        _, y, _ = ids_of(ids_ref)
        pick = token_weights(table_ref[...], cap)
        picks = [pick(index) for index in range(len(parts))]
        for j in range(y_count):
            column = pl.ds(pl.multiple_of(jnp.bitwise_xor(y, j) * width, width), width)
            total = dot(picks[0], ins[0][:, column])
            for index in range(1, len(parts)):
                total = total + dot(picks[index], ins[index][:, column])
            outs[j][...] = total.astype(outs[j].dtype)

    outs = [sds((tokens, width), F32)] + [sds((tokens, width), BF)] * (y_count - 1)
    return call(body, "near_combine", ids, (table, *parts), outs)


def final_combine(ids, parts, near_keep, near_received, table, sizes):
    experts, cap, width, y_count = sizes
    tokens = table.shape[0]
    half = experts // 2

    def body(ids_ref, table_ref, keep_ref, *refs):
        received, ins, out_ref = refs[: y_count - 1], refs[y_count - 1 : -1], refs[-1]
        pick = token_weights(table_ref[...], cap)
        total = keep_ref[...]
        for ref in received:
            total = total + ref[...].astype(F32)
        for index in range(half):
            total = total + dot(pick(half + index), ins[index][...])
        out_ref[...] = total.astype(BF)

    return call(
        body,
        "final_combine",
        ids,
        (table, near_keep, *near_received, *parts),
        [sds((tokens, width), BF)],
    )[0]


def swap(value, axis, step):
    count = lax.axis_size(axis)
    return lax.ppermute(value, axis, [(i, i ^ step) for i in range(count)])


def tall(rows):
    return jnp.transpose(fill_rows(rows))


def conv_block(signal, rim_t, taps_t):
    kinds = [taps_t[k : k + 1, :] for k in range(taps_t.shape[0])]
    taps = tall(kinds)
    count = len(kinds)
    place = lax.broadcasted_iota(jnp.int32, (16, 128), 0)
    lane = lax.broadcasted_iota(jnp.int32, (16, 128), 1)
    put = ((lane == place + 125) & (place < 3)).astype(F32).astype(BF)
    edge = dot(jnp.transpose(rim_t.astype(F32)).astype(BF), put)
    value = signal.astype(F32)
    joined = jnp.concatenate([edge, value], axis=1)
    total = taps[:, count - 1 : count] * value
    for back in range(1, count):
        total = total + taps[:, count - 1 - back : count - back] * pltpu.roll(joined, back, 1)[:, 128:]
    return silu(total)


def head_rows(table, heads_here, length):
    return jnp.concatenate(
        [jnp.broadcast_to(table[i : i + 1, :], (HEAD_DIM, length)) for i in range(heads_here)], axis=0
    )


def mixer_open(ids, x_in, dt_raw, rate_row, b_in, c_in, taps_x, taps_b, taps_c, rims, weights, hb, hp, y_count):
    rows, length = x_in.shape
    heads = dt_raw.shape[0]
    block_rows = hb * HEAD_DIM

    def body(ids_ref, x_ref, dt_ref, rate_ref, b_ref, c_ref, tx_ref, tb_ref, tc_ref, rim_ref, *refs):
        from_refs, outs = refs[: len(weights)], refs[len(weights) :]
        xs_ref, cum_ref, bt_ref, conv_c_ref, msg_ref = outs[:5]
        into_refs, (step_ref, sems) = outs[5:-2], outs[-2:]
        copies = [
            pltpu.make_async_copy(source, target, sems.at[index])
            for index, (source, target) in enumerate(zip(from_refs, into_refs))
        ]
        _, y, _ = ids_of(ids_ref)
        turn = pl.program_id(0)

        @pl.when(turn == 0)
        def _():
            for copy in copies:
                copy.start()
            group = y * (GROUPS * 2) // (2 * y_count)
            start = pl.multiple_of(group * NSTATE, NSTATE)
            span = pl.ds(start, NSTATE)
            b_conv = conv_block(b_ref[span, :], rim_ref[:, rows : rows + NSTATE], tb_ref[:, span])
            c_conv = conv_block(c_ref[span, :], rim_ref[:, rows + NSTATE :], tc_ref[:, span])
            bt_ref[...] = jnp.transpose(b_conv).astype(BF)
            conv_c_ref[...] = c_conv.astype(BF)
            raw = dt_ref[...]
            step = jnp.maximum(raw, 0.0) + jnp.log1p(jnp.exp(-jnp.abs(raw)))
            eye_r = lax.broadcasted_iota(jnp.int32, (heads, heads), 0)
            eye_c = lax.broadcasted_iota(jnp.int32, (heads, heads), 1)
            rate = jnp.sum(jnp.where(eye_r == eye_c, rate_ref[...], 0.0), axis=1, keepdims=True)
            cum = -step * rate
            lane = lax.broadcasted_iota(jnp.int32, (heads, length), 1)
            shift = 1
            while shift < length:
                cum = cum + jnp.where(lane >= shift, pltpu.roll(cum, shift, 1), 0.0)
                shift *= 2
            step_ref[...] = step
            cum_ref[...] = cum
            total = jnp.broadcast_to(jnp.exp(cum[:, length - 1 : length]), (heads, NSTATE))
            if heads < hp:
                total = jnp.concatenate([total, jnp.ones((hp - heads, NSTATE), F32)], axis=0)
            high = total.astype(BF)
            msg_ref[rows : rows + hp, :] = high
            msg_ref[rows + hp : rows + 2 * hp, :] = (total - high.astype(F32)).astype(BF)

        value = conv_block(x_ref[...], rim_ref[:, pl.ds(pl.multiple_of(turn * block_rows, block_rows), block_rows)], tx_ref[...])
        first = turn * hb if heads > hb else 0
        step = step_ref[pl.ds(first, hb), :]
        cum = cum_ref[pl.ds(first, hb), :]
        fade = jnp.exp(cum[:, length - 1 : length] - cum)
        scaled = value * head_rows(step, hb, length)
        xs_ref[...] = scaled.astype(BF)
        state = dot((scaled * head_rows(fade, hb, length)).astype(BF), bt_ref[...])
        msg_ref[pl.ds(pl.multiple_of(turn * block_rows, block_rows), block_rows), :] = state.astype(BF)

        @pl.when(turn == heads // hb - 1)
        def _():
            for copy in copies:
                copy.wait()

    outs = [
        sds((rows, length), BF),
        sds((heads, length), F32),
        sds((length, NSTATE), BF),
        sds((NSTATE, length), BF),
        sds((rows + 2 * hp, NSTATE), BF),
    ] + [sds(w.shape, w.dtype) for w in weights]
    vmem = pl.BlockSpec(memory_space=pltpu.VMEM)
    return call(
        body,
        "mixer_open",
        ids,
        (*map(in_hbm, (x_in, dt_raw, rate_row, b_in, c_in, taps_x, taps_b, taps_c)), rims, *map(in_hbm, weights)),
        outs,
        grid=(heads // hb,),
        in_specs=[
            pl.BlockSpec((block_rows, length), lambda i, s: (i, 0)),
            whole(dt_raw.shape),
            whole(rate_row.shape),
            whole(b_in.shape),
            whole(c_in.shape),
            pl.BlockSpec((taps_x.shape[0], block_rows), lambda i, s: (0, i)),
            whole(taps_b.shape),
            whole(taps_c.shape),
            vmem,
        ]
        + [pl.BlockSpec(memory_space=pltpu.HBM)] * len(weights),
        out_specs=[pl.BlockSpec((block_rows, length), lambda i, s: (i, 0))]
        + [whole(o.shape) for o in outs[1:5]]
        + [vmem] * len(weights),
        scratch=[pltpu.VMEM((heads, length), F32), pltpu.SemaphoreType.DMA((len(weights),))],
        us=7.0,
        mib=OPEN_MIB,
    )


def per_row(table, heads):
    width = table.shape[1]
    return jnp.broadcast_to(table[:heads][:, None, :], (heads, HEAD_DIM, width)).reshape(
        heads * HEAD_DIM, width
    )


def state_round(ids, mine, received, carried, level, heads, hp):
    rows = heads * HEAD_DIM
    opening = carried is None
    outs = [sds(mine.shape, BF), sds((rows, NSTATE), F32), sds((hp, NSTATE), F32)]

    def body(ids_ref, mine_ref, recv_ref, *refs):
        msg_ref, pre_ref, dec_ref = refs[-3:]
        upper = (ids_ref[0] >> level) % 2 == 1
        t_mine = mine_ref[:rows, :].astype(F32)
        t_recv = recv_ref[:rows, :].astype(F32)

        def decay(ref):
            return ref[rows : rows + hp, :].astype(F32) + ref[rows + hp :, :].astype(F32)

        d_mine, d_recv = decay(mine_ref), decay(recv_ref)
        one = jnp.ones_like(d_mine)
        d_late = jnp.where(upper, d_mine, d_recv)
        late = jnp.where(upper, t_mine, t_recv)
        early = jnp.where(upper, t_recv, t_mine)
        total = late + per_row(d_late, heads) * early
        msg_ref[:rows, :] = total.astype(BF)
        both = d_mine * d_recv
        high = both.astype(BF)
        msg_ref[rows : rows + hp, :] = high
        msg_ref[rows + hp :, :] = (both - high.astype(F32)).astype(BF)
        if opening:
            pre_ref[...] = jnp.where(upper, t_recv, jnp.zeros_like(t_recv))
            dec_ref[...] = jnp.where(upper, d_recv, one)
        else:
            old_pre, old_dec = refs[0], refs[1]
            grown = old_pre[...] + per_row(old_dec[...], heads) * t_recv
            pre_ref[...] = jnp.where(upper, grown, old_pre[...])
            dec_ref[...] = jnp.where(upper, old_dec[...] * d_recv, old_dec[...])

    ins = (mine, received) if opening else (mine, received, *carried)
    return call(body, f"state_round_{level}", ids, ins, outs)


def mixer_close(ids, carried, received, xs, cum, b_t, c_conv, z_in, gain_row, hb):
    rows, length = xs.shape
    heads = cum.shape[0]
    block_rows = hb * HEAD_DIM
    blocks = length // BLOCK

    def body(ids_ref, pre_ref, dec_ref, recv_ref, xs_ref, cum_ref, bt_ref, c_ref, z_ref, gain_ref, out_ref, gram_ref, y_ref):
        turn = pl.program_id(0)

        @pl.when(turn == 0)
        def _():
            row = lax.broadcasted_iota(jnp.int32, (BLOCK, BLOCK), 0)
            col = lax.broadcasted_iota(jnp.int32, (BLOCK, BLOCK), 1)
            for j in range(blocks):
                span = slice(j * BLOCK, (j + 1) * BLOCK)
                gram = dot(bt_ref[span, :], c_ref[:, span])
                gram_ref[j] = jnp.where(row <= col, gram, 0.0)

        first = turn * hb if heads > hb else 0
        decay = dec_ref[pl.ds(first, hb), :]
        own = pl.ds(pl.multiple_of(turn * block_rows, block_rows), block_rows)
        state = pre_ref[own, :] + head_rows(decay, hb, NSTATE) * recv_ref[own, :].astype(F32)
        cum = cum_ref[...]
        down_cum = jnp.transpose(fill_rows([cum[i : i + 1, :] for i in range(hb)]))
        before = jnp.zeros((hb, 1), F32)
        for j in range(blocks):
            span = slice(j * BLOCK, (j + 1) * BLOCK)
            here = cum[:, span]
            after = here[:, BLOCK - 1 : BLOCK]
            c_block = c_ref[:, span]
            flow = dot(state.astype(BF), c_block) * head_rows(jnp.exp(here - before), hb, BLOCK)
            gram = gram_ref[j]
            for i in range(hb):
                lines = slice(i * HEAD_DIM, (i + 1) * HEAD_DIM)
                gap = jnp.minimum(here[i : i + 1, :] - down_cum[span, i : i + 1], 0.0)
                mask = (gram * jnp.exp(gap)).astype(BF)
                y_ref[lines, span] = flow[lines, :] + dot(xs_ref[lines, span], mask)
            if j + 1 < blocks:
                fade = head_rows(jnp.exp(after - here), hb, BLOCK)
                fresh = dot((xs_ref[:, span].astype(F32) * fade).astype(BF), bt_ref[span, :])
                kept = head_rows(jnp.broadcast_to(jnp.exp(after - before), (hb, NSTATE)), hb, NSTATE)
                state = kept * state + fresh
            before = after
        gain = tall([gain_ref[...]])
        for i in range(hb):
            lines = slice(i * HEAD_DIM, (i + 1) * HEAD_DIM)
            gated = y_ref[lines, :] * silu(z_ref[lines, :].astype(F32))
            scale = lax.rsqrt(jnp.mean(gated * gated, axis=0, keepdims=True) + HEAD_EPS)
            out_ref[lines, :] = (gated * scale * gain[lines, 0:1]).astype(BF)

    pre, dec = carried
    tile = pl.BlockSpec((block_rows, length), lambda i, s: (i, 0))
    vmem = pl.BlockSpec(memory_space=pltpu.VMEM)
    return call(
        body,
        "mixer_close",
        ids,
        (pre, dec, received, xs, cum, b_t, c_conv, in_hbm(z_in), in_hbm(gain_row)),
        [sds((rows, length), BF)],
        grid=(heads // hb,),
        in_specs=[
            vmem,
            vmem,
            vmem,
            tile,
            pl.BlockSpec((hb, length), lambda i, s: (i, 0)),
            whole(b_t.shape),
            whole(c_conv.shape),
            tile,
            pl.BlockSpec((1, block_rows), lambda i, s: (0, i)),
        ],
        out_specs=[tile],
        scratch=[pltpu.VMEM((blocks, BLOCK, BLOCK), F32), pltpu.VMEM((block_rows, length), F32)],
        us=6.0,
        mib=12,
    )[0]


def block(
    x_in,
    z_in,
    dt_raw,
    decay_rate,
    b_in,
    c_in,
    conv_x,
    conv_b,
    conv_c,
    head_gain,
    moe_rows,
    moe_gain,
    routes,
    route_logit,
    w_gate,
    w_up,
    w_down,
):
    ep, tp = lax.axis_size("ep"), lax.axis_size("tp")
    y_count = tp // 2
    heads = dt_raw.shape[0]
    hb, hp = min(8, heads), -(-heads // 16) * 16
    tokens, features = moe_rows.shape
    experts = ep * w_gate.shape[0]
    capacity = 2 * tokens * routes.shape[1] // experts
    cap = -(-capacity // 16) * 16
    sizes = (experts, cap, features // tp, y_count)
    half = experts // 2
    ids = jnp.stack([lax.axis_index("ep"), lax.axis_index("tp")]).astype(jnp.int32)
    routes_t, logit_t = routes.T, route_logit.T

    outs = prep(ids, moe_rows, moe_gain.reshape(1, -1), routes_t, logit_t, x_in, b_in, c_in, sizes)
    self_rows, near, far = outs[0], outs[1:half], outs[half : 2 * half]
    table, own_rims = outs[-2:]
    rims = lax.ppermute(own_rims, "ep", [(i, i + 1) for i in range(ep - 1)])
    far = [swap(value, "ep", half + index) for index, value in enumerate(far)]
    near = [swap(value, "ep", 1 + index) for index, value in enumerate(near)]
    far_sets = []
    for part in range(2):
        mine = far[part * half // 2 : (part + 1) * half // 2]
        value = jnp.concatenate(mine, axis=0)
        far_sets.append([value] + [swap(value, "tp", 2 * j) for j in range(1, y_count)])
    near_other = [swap(value, "tp", 1) for value in near]
    far_other = [[swap(value, "tp", 1) for value in group] for group in far_sets]

    xs, cum, b_t, c_conv, message, w_gate, w_up = mixer_open(
        ids,
        x_in,
        dt_raw,
        decay_rate.reshape(1, -1),
        b_in,
        c_in,
        conv_x.T,
        conv_b.T,
        conv_c.T,
        rims,
        (w_gate, w_up),
        hb,
        hp,
        y_count,
    )
    carried, level = None, 0
    while (2 << level) < ep:
        received = swap(message, "ep", 1 << level)
        message, *carried = state_round(ids, message, received, carried, level, heads, hp)
        level += 1
    top = 1 << level
    last = lax.ppermute(message, "ep", [(i, i + top) for i in range(ep - top)])

    hid_near, hid_far, w_down = gate_up(
        ids, self_rows, near, near_other, far_sets, far_other, w_gate, w_up, w_down, sizes
    )
    send_far, keep_far = down(ids, hid_far, w_down, sizes, "down_far")
    recv_far = swap(send_far, "tp", 1)
    send_near, keep_near = down(ids, hid_near, w_down, sizes, "down_near")
    recv_near = swap(send_near, "tp", 1)
    near_out = near_sum(ids, keep_near, recv_near, sizes)
    near_back = [near_out[0]] + [swap(near_out[k], "ep", k) for k in range(1, half)]
    far_outs = far_split(ids, keep_far, recv_far, sizes)
    far_back = []
    for part in range(2):
        far_keep, *far_send = far_outs[part * y_count : (part + 1) * y_count]
        label = "ab"[part]
        far_parts = [far_keep] + [
            swap(value, "tp", 2 * (j + 1)) for j, value in enumerate(far_send)
        ]
        far_out = far_sum(ids, far_parts, sizes, "far_sum_" + label)
        first = half + part * (half // 2)
        far_back += [swap(value, "ep", first + index) for index, value in enumerate(far_out)]
    outs = near_combine(ids, near_back, table, sizes)
    near_keep = outs[0]
    near_received = [swap(value, "tp", 2 * (j + 1)) for j, value in enumerate(outs[1:])]
    moe_t = final_combine(ids, far_back, near_keep, near_received, table, sizes)

    mixed = mixer_close(
        ids, carried, last, xs, cum, b_t, c_conv, z_in, head_gain.reshape(1, -1), hb
    )
    return (mixed, moe_t.T)


def solution(mesh):
    return jax.shard_map(
        block,
        mesh=mesh,
        in_specs=(
            P("tp", "ep"),
            P("tp", "ep"),
            P("tp", "ep"),
            P("tp"),
            P(None, "ep"),
            P(None, "ep"),
            P("tp", None),
            P(),
            P(),
            P("tp"),
            P("ep", None),
            P(),
            P("ep", None),
            P("ep", None),
            P("ep", None, "tp"),
            P("ep", None, "tp"),
            P("ep", "tp", None),
        ),
        out_specs=(P("tp", "ep"), P("tp", "ep")),
        check_vma=False,
    )
```

```python
import jax
import jax.numpy as jnp
from jax import lax
from jax.experimental import pallas as pl
from jax.experimental.pallas import tpu as pltpu
from jax.sharding import PartitionSpec as P


HEAD_DIM = 64
GROUPS = 2
NSTATE = 128
BLOCK = 128
ROW_EPS = 0.1
HEAD_EPS = 1.0

BF = jnp.bfloat16
F32 = jnp.float32


def sds(shape, dtype):
    return jax.ShapeDtypeStruct(shape, dtype)


def dot(a, b):
    return jnp.dot(a, b, preferred_element_type=F32)


def silu(v):
    return v * (0.5 + 0.5 * jnp.tanh(0.5 * v))


def call(body, name, ids, *args, **kwargs):
    return launch(body, name, ids, *args, **kwargs)


def launch(body, name, ids, ins, outs, grid=None, in_specs=None, out_specs=None, scratch=(), us=1.0, mib=6):
    vmem = pl.BlockSpec(memory_space=pltpu.VMEM)
    common = dict(
        name=name,
        out_shape=outs,
        cost_estimate=pl.CostEstimate(
            flops=int(us * 2.5e8), bytes_accessed=0, transcendentals=0
        ),
    )
    limit = mib * 1024 * 1024
    if grid is None:
        return pl.pallas_call(
            body,
            in_specs=[pl.BlockSpec(memory_space=pltpu.SMEM)] + (in_specs or [vmem] * len(ins)),
            out_specs=out_specs or [vmem] * len(outs),
            scratch_shapes=list(scratch),
            compiler_params=pltpu.CompilerParams(vmem_limit_bytes=limit),
            **common,
        )(ids, *ins)
    return pl.pallas_call(
        body,
        grid_spec=pltpu.PrefetchScalarGridSpec(
            num_scalar_prefetch=1,
            grid=grid,
            in_specs=in_specs,
            out_specs=out_specs,
            scratch_shapes=list(scratch),
        ),
        compiler_params=pltpu.CompilerParams(
            dimension_semantics=("arbitrary",) * len(grid), vmem_limit_bytes=limit
        ),
        **common,
    )(ids, *ins)


GATE_MIB = 24
DOWN_MIB = 16
OPEN_MIB = 28


def in_hbm(value):
    return pltpu.with_memory_space_constraint(value, pltpu.HBM)


def ids_of(ids_ref):
    place, column = ids_ref[0], ids_ref[1]
    return place, column // 2, column % 2


def fill_rows(rows, count=8):
    width = rows[0].shape[1]
    at = lax.broadcasted_iota(jnp.int32, (count, width), 0)
    out = jnp.broadcast_to(rows[0], (count, width))
    for index in range(1, len(rows)):
        out = jnp.where(at == index, rows[index], out)
    return out


def destinations(routes_t, place, experts, capacity):
    tokens = routes_t.shape[1]
    relative = jnp.bitwise_xor(routes_t, place)
    first, second = relative[0:1, :], relative[1:2, :]
    at = lax.broadcasted_iota(jnp.int32, (experts, tokens), 0)
    hit_a = (at == first).astype(F32)
    hit_b = (at == second).astype(F32)
    row = lax.broadcasted_iota(jnp.int32, (tokens, tokens), 0)
    col = lax.broadcasted_iota(jnp.int32, (tokens, tokens), 1)
    before = (row < col).astype(F32).astype(BF)
    ahead = dot((hit_a + hit_b).astype(BF), before)
    rank_a = jnp.sum(hit_a * ahead, axis=0, keepdims=True).astype(jnp.int32)
    rank_b = jnp.sum(hit_b * ahead, axis=0, keepdims=True).astype(jnp.int32)
    return first * capacity + rank_a, second * capacity + rank_b


def prep(ids, moe_rows, moe_gain, routes_t, logit_t, mixer_args, sizes):
    x_in, b_in, _ = mixer_args[:3]
    tokens, features = moe_rows.shape
    experts, cap, width, y_count = sizes
    half = experts // 2
    value_rows, length = x_in.shape
    group_rows = b_in.shape[0] // GROUPS

    def body(ids_ref, rows_hbm, gain_hbm, routes_hbm, logit_hbm, *refs):
        count = len(mixer_args)
        mixer_hbm, outs, scratch = refs[:count], refs[count:-6], refs[-6:]
        normed_ref, sems = scratch[0], scratch[-1]
        rows_ref, gain_ref, routes_ref, logit_ref = scratch[1:-1]
        self_ref, near, far = outs[0], outs[1:half], outs[half : 2 * half]
        table_ref, rim_ref = outs[2 * half : 2 * half + 2]
        mixer_vmem = outs[2 * half + 2 :]
        x_ref, b_ref, c_ref = mixer_vmem[:3]
        place, y, core = ids_of(ids_ref)
        tail = slice(length - 128, length)
        moves = (
            (rows_hbm, rows_ref),
            (gain_hbm, gain_ref),
            (routes_hbm, routes_ref),
            (logit_hbm, logit_ref),
            *zip(mixer_hbm, mixer_vmem),
        )
        copies = [
            pltpu.make_async_copy(source, target, sems.at[index])
            for index, (source, target) in enumerate(moves)
        ]
        for copy in copies:
            copy.start()
        for copy in copies[:4]:
            copy.wait()
        rows = rows_ref[...].astype(F32)
        scale = lax.rsqrt(jnp.mean(rows * rows, axis=1, keepdims=True) + ROW_EPS)
        normed_ref[...] = (rows * scale * gain_ref[...]).astype(BF)
        dest_a, dest_b = destinations(routes_ref[...], place, experts, cap)

        def pick(index):
            slot = lax.broadcasted_iota(jnp.int32, (cap, tokens), 0) + index * cap
            return ((slot == dest_a) | (slot == dest_b)).astype(F32).astype(BF)

        def columns(block):
            return normed_ref[:, pl.ds(pl.multiple_of(block * width, width), width)]

        mine = columns(2 * y + core)
        for index in range(half):
            far[index][...] = dot(pick(half + index), mine).astype(BF)
        for j in range(y_count):
            part = columns(2 * j + core)
            for index in range(1, half):
                near[index - 1][:, j * width : (j + 1) * width] = dot(pick(index), part).astype(BF)
        self_ref[...] = dot(pick(0), normed_ref[...]).astype(BF)
        gap = logit_ref[0:1, :] - logit_ref[1:2, :]
        shares = [jax.nn.sigmoid(gap), jax.nn.sigmoid(-gap)]
        table_ref[...] = jnp.transpose(
            fill_rows([dest_a.astype(F32), dest_b.astype(F32)] + shares)
        )
        for copy in copies[4:]:
            copy.wait()
        group = y * (GROUPS * 2) // (2 * y_count)
        start = pl.multiple_of(group * group_rows, group_rows)
        line = lax.broadcasted_iota(jnp.int32, (16, 128), 0)
        lane = lax.broadcasted_iota(jnp.int32, (16, 128), 1)
        take = (lane == line + 125).astype(F32).astype(BF)
        nt = (((1,), (1,)), ((), ()))

        def edge(block):
            return lax.dot_general(take, block, nt, preferred_element_type=F32).astype(BF)

        rim_ref[:, :value_rows] = edge(x_ref[:, tail])
        rim_ref[:, value_rows : value_rows + group_rows] = edge(b_ref[pl.ds(start, group_rows), tail])
        rim_ref[:, value_rows + group_rows :] = edge(c_ref[pl.ds(start, group_rows), tail])

    outs = [sds((cap, features), BF)]
    outs += [sds((cap, y_count * width), BF)] * (half - 1)
    outs += [sds((cap, width), BF)] * half
    outs += [sds((tokens, 8), F32), sds((16, value_rows + 2 * group_rows), BF)]
    outs += [sds(a.shape, a.dtype) for a in mixer_args]
    return call(
        body,
        "prep",
        ids,
        tuple(map(in_hbm, (moe_rows, moe_gain, routes_t, logit_t, *mixer_args))),
        outs,
        in_specs=[pl.BlockSpec(memory_space=pltpu.HBM)] * (4 + len(mixer_args)),
        scratch=[
            pltpu.VMEM((tokens, features), BF),
            pltpu.VMEM(moe_rows.shape, BF),
            pltpu.VMEM(moe_gain.shape, F32),
            pltpu.VMEM(routes_t.shape, jnp.int32),
            pltpu.VMEM(logit_t.shape, F32),
            pltpu.SemaphoreType.DMA((4 + len(mixer_args),)),
        ],
        us=3.0,
        mib=10,
    )


def gate_up(ids, self_rows, near, near_other, far, far_other, w_gate, w_up, w_down, z_in, sizes):
    experts, cap, width, y_count = sizes
    features, hidden = w_gate.shape[1:]
    rows = experts * cap
    split = experts // 2 * cap
    step = 256 if hidden % 256 == 0 else hidden
    groups = (near, near_other, *far, *far_other)
    pieces = (self_rows, *(value for group in groups for value in group))

    def body(ids_ref, *refs):
        wg_ref, wu_ref, wd_ref, z_ref, low_ref, high_ref, held_ref, held_z_ref, lhs_ref, sems = refs[len(pieces) :]
        copies = [
            pltpu.make_async_copy(wd_ref, held_ref, sems.at[0]),
            pltpu.make_async_copy(z_ref, held_z_ref, sems.at[1]),
        ]
        for copy in copies:
            copy.start()
        at, held = 1, []
        for group in groups:
            held.append(refs[at : at + len(group)])
            at += len(group)
        _, y, core = ids_of(ids_ref)

        def columns(block):
            return pl.ds(pl.multiple_of(block * width, width), width)

        lhs_ref[0:cap, :] = refs[0][...]
        for source, c in ((held[0], core), (held[1], 1 - core)):
            for index, ref in enumerate(source):
                lines = slice(cap * (1 + index), cap * (2 + index))
                for j in range(y_count):
                    lhs_ref[lines, columns(2 * j + c)] = ref[:, j * width : (j + 1) * width]
        for set_at, c in ((2, core), (2 + len(far), 1 - core)):
            start = split
            for source in held[set_at : set_at + len(far)]:
                tall_rows = source[0].shape[0]
                for j, ref in enumerate(source):
                    lines = slice(start, start + tall_rows)
                    lhs_ref[lines, columns(2 * jnp.bitwise_xor(y, j) + c)] = ref[...]
                start += tall_rows

        for turn in range(hidden // step):
            span = slice(turn * step, (turn + 1) * step)
            for lines, out_ref in ((slice(0, split), low_ref), (slice(split, rows), high_ref)):
                lhs = lhs_ref[lines, :]
                gate = dot(lhs, wg_ref[0, :, span])
                up = dot(lhs, wu_ref[0, :, span])
                out_ref[:, span] = (silu(gate) * up).astype(BF)
        for copy in copies:
            copy.wait()

    vmem = pl.BlockSpec(memory_space=pltpu.VMEM)
    return call(
        body,
        "gate_up",
        ids,
        (*pieces, w_gate, w_up, in_hbm(w_down), in_hbm(z_in)),
        [sds((split, hidden), BF)] * 2 + [sds(w_down.shape, BF), sds(z_in.shape, BF)],
        in_specs=[vmem] * (len(pieces) + 2) + [pl.BlockSpec(memory_space=pltpu.HBM)] * 2,
        scratch=[pltpu.VMEM((rows, features), BF), pltpu.SemaphoreType.DMA((2,))],
        us=9.0,
        mib=GATE_MIB,
    )


def down(ids, hidden, w_down, sizes, name):
    _, _, width, y_count = sizes
    rows, _ = hidden.shape

    def body(ids_ref, h_ref, w_ref, send_ref, keep_ref):
        core = ids_ref[1] % 2
        for out_ref, c in ((send_ref, 1 - core), (keep_ref, core)):
            for j in range(y_count):
                column = pl.ds(pl.multiple_of((2 * j + c) * width, width), width)
                value = dot(h_ref[...], w_ref[0, :, column])
                out_ref[:, j * width : (j + 1) * width] = value.astype(BF)

    return call(
        body,
        name,
        ids,
        (hidden, w_down),
        [sds((rows, y_count * width), BF)] * 2,
        us=2.0,
        mib=DOWN_MIB,
    )


def near_sum(ids, keep, received, sizes):
    experts, cap, width, y_count = sizes
    half = experts // 2

    def body(ids_ref, keep_ref, recv_ref, *outs):
        for index in range(half):
            span = pl.ds(index * cap, cap)
            outs[index][...] = (
                keep_ref[span, :].astype(F32) + recv_ref[span, :].astype(F32)
            ).astype(BF)

    outs = [sds((cap, y_count * width), BF)] * half
    return call(body, "near_sum", ids, (keep, received), outs)


def far_split(ids, keep, received, sizes):
    _, _, width, y_count = sizes
    rows = keep.shape[0]

    def body(ids_ref, keep_ref, recv_ref, *outs):
        _, y, _ = ids_of(ids_ref)
        for part in range(2):
            lines = pl.ds(part * rows // 2, rows // 2)
            for j in range(y_count):
                column = pl.ds(pl.multiple_of(jnp.bitwise_xor(y, j) * width, width), width)
                outs[part * y_count + j][...] = (
                    keep_ref[lines, column].astype(F32) + recv_ref[lines, column].astype(F32)
                ).astype(BF)

    outs = [sds((rows // 2, width), BF)] * (2 * y_count)
    return call(body, "far_split", ids, (keep, received), outs)


def far_sum(ids, parts, sizes, name):
    experts, cap, width, _ = sizes
    count = experts // 4

    def body(ids_ref, *refs):
        ins, outs = refs[: len(parts)], refs[len(parts) :]
        for index in range(count):
            span = pl.ds(index * cap, cap)
            total = ins[0][span, :].astype(F32)
            for ref in ins[1:]:
                total = total + ref[span, :].astype(F32)
            outs[index][...] = total.astype(BF)

    return call(body, name, ids, parts, [sds((cap, width), BF)] * count)


def token_weights(table, cap):
    tokens = table.shape[0]
    first, second = table[:, 0:1], table[:, 1:2]
    share_a, share_b = table[:, 2:3], table[:, 3:4]

    def pick(index):
        slot = (lax.broadcasted_iota(jnp.int32, (tokens, cap), 1) + index * cap).astype(F32)
        return (
            jnp.where(slot == first, share_a, 0.0) + jnp.where(slot == second, share_b, 0.0)
        ).astype(BF)

    return pick


def near_combine(ids, parts, table, sizes):
    _, cap, width, y_count = sizes
    tokens = table.shape[0]

    def body(ids_ref, table_ref, *refs):
        ins, outs = refs[: len(parts)], refs[len(parts) :]
        _, y, _ = ids_of(ids_ref)
        pick = token_weights(table_ref[...], cap)
        picks = [pick(index) for index in range(len(parts))]
        for j in range(y_count):
            column = pl.ds(pl.multiple_of(jnp.bitwise_xor(y, j) * width, width), width)
            total = dot(picks[0], ins[0][:, column])
            for index in range(1, len(parts)):
                total = total + dot(picks[index], ins[index][:, column])
            outs[j][...] = total.astype(outs[j].dtype)

    outs = [sds((tokens, width), F32)] + [sds((tokens, width), BF)] * (y_count - 1)
    return call(body, "near_combine", ids, (table, *parts), outs)


def final_combine(ids, parts, near_keep, near_received, table, sizes):
    experts, cap, width, y_count = sizes
    tokens = table.shape[0]
    half = experts // 2

    def body(ids_ref, table_ref, keep_ref, *refs):
        received, ins, out_ref = refs[: y_count - 1], refs[y_count - 1 : -1], refs[-1]
        pick = token_weights(table_ref[...], cap)
        total = keep_ref[...]
        for ref in received:
            total = total + ref[...].astype(F32)
        for index in range(half):
            total = total + dot(pick(half + index), ins[index][...])
        out_ref[...] = total.astype(BF)

    return call(
        body,
        "final_combine",
        ids,
        (table, near_keep, *near_received, *parts),
        [sds((tokens, width), BF)],
    )[0]


def swap(value, axis, step):
    count = lax.axis_size(axis)
    return lax.ppermute(value, axis, [(i, i ^ step) for i in range(count)])


def tall(rows):
    return jnp.transpose(fill_rows(rows))


def conv_block(signal, rim_t, taps_t):
    kinds = [taps_t[k : k + 1, :] for k in range(taps_t.shape[0])]
    taps = tall(kinds)
    count = len(kinds)
    place = lax.broadcasted_iota(jnp.int32, (16, 128), 0)
    lane = lax.broadcasted_iota(jnp.int32, (16, 128), 1)
    put = ((lane == place + 125) & (place < 3)).astype(F32).astype(BF)
    edge = dot(jnp.transpose(rim_t.astype(F32)).astype(BF), put)
    value = signal.astype(F32)
    joined = jnp.concatenate([edge, value], axis=1)
    total = taps[:, count - 1 : count] * value
    for back in range(1, count):
        total = total + taps[:, count - 1 - back : count - back] * pltpu.roll(joined, back, 1)[:, 128:]
    return silu(total)


def head_rows(table, heads_here, length):
    return jnp.concatenate(
        [jnp.broadcast_to(table[i : i + 1, :], (HEAD_DIM, length)) for i in range(heads_here)], axis=0
    )


def sent_decay(total, hp):
    count, width = total.shape
    if count < hp:
        total = jnp.concatenate([total, jnp.ones((hp - count, width), F32)], axis=0)
    high = total.astype(BF)
    return high, (total - high.astype(F32)).astype(BF)


def decay_of(ref, rows, hp):
    return ref[rows : rows + hp, :].astype(F32) + ref[rows + hp :, :].astype(F32)


def span_state(signal, rim, taps, step, cum, b_t, xs_ref, msg_ref, hb, hp):
    rows, length = signal.shape
    value = conv_block(signal, rim, taps)
    last = cum[:, length - 1 : length]
    scaled = value * head_rows(step, hb, length)
    xs_ref[...] = scaled.astype(BF)
    state = dot((scaled * head_rows(jnp.exp(last - cum), hb, length)).astype(BF), b_t)
    msg_ref[:rows, :] = state.astype(BF)
    high, low = sent_decay(jnp.broadcast_to(jnp.exp(last), (hb, NSTATE)), hp)
    msg_ref[rows : rows + hp, :] = high
    msg_ref[rows + hp :, :] = low


def mixer_open_a(ids, x_in, dt_raw, rate_row, b_in, c_in, taps_x, taps_b, taps_c, rims, weight, hb, hp, y_count):
    rows, length = x_in.shape
    heads = dt_raw.shape[0]
    part = hb * HEAD_DIM

    def body(ids_ref, x_ref, dt_ref, rate_ref, b_ref, c_ref, tx_ref, tb_ref, tc_ref, rim_ref, w_ref, *outs):
        xs_ref, cum_a_ref, cum_b_ref, step_ref, bt_ref, conv_c_ref, msg_ref, into_ref, sem = outs
        copy = pltpu.make_async_copy(w_ref, into_ref, sem)
        copy.start()
        _, y, _ = ids_of(ids_ref)
        group = y * (GROUPS * 2) // (2 * y_count)
        start = pl.multiple_of(group * NSTATE, NSTATE)
        span = pl.ds(start, NSTATE)
        b_conv = conv_block(b_ref[span, :], rim_ref[:, rows : rows + NSTATE], tb_ref[:, span])
        c_conv = conv_block(c_ref[span, :], rim_ref[:, rows + NSTATE :], tc_ref[:, span])
        b_t = jnp.transpose(b_conv).astype(BF)
        bt_ref[...] = b_t
        conv_c_ref[...] = c_conv.astype(BF)
        raw = dt_ref[...]
        step = jnp.maximum(raw, 0.0) + jnp.log1p(jnp.exp(-jnp.abs(raw)))
        eye_r = lax.broadcasted_iota(jnp.int32, (heads, heads), 0)
        eye_c = lax.broadcasted_iota(jnp.int32, (heads, heads), 1)
        rate = jnp.sum(jnp.where(eye_r == eye_c, rate_ref[...], 0.0), axis=1, keepdims=True)
        cum = -step * rate
        lane = lax.broadcasted_iota(jnp.int32, (heads, length), 1)
        shift = 1
        while shift < length:
            cum = cum + jnp.where(lane >= shift, pltpu.roll(cum, shift, 1), 0.0)
            shift *= 2
        step_ref[...] = step[hb:]
        cum_a_ref[...] = cum[:hb]
        cum_b_ref[...] = cum[hb:]
        span_state(x_ref[:part, :], rim_ref[:, :part], tx_ref[:, :part], step[:hb], cum[:hb], b_t, xs_ref, msg_ref, hb, hp)
        copy.wait()

    vmem = pl.BlockSpec(memory_space=pltpu.VMEM)
    outs = [
        sds((part, length), BF),
        sds((hb, length), F32),
        sds((hb, length), F32),
        sds((hb, length), F32),
        sds((length, NSTATE), BF),
        sds((NSTATE, length), BF),
        sds((part + 2 * hp, NSTATE), BF),
        sds(weight.shape, weight.dtype),
    ]
    return call(
        body,
        "mixer_open_a",
        ids,
        (x_in, dt_raw, rate_row, b_in, c_in, taps_x, taps_b, taps_c, rims, in_hbm(weight)),
        outs,
        in_specs=[vmem] * 9 + [pl.BlockSpec(memory_space=pltpu.HBM)],
        out_specs=[vmem] * len(outs),
        scratch=[pltpu.SemaphoreType.DMA],
        us=4.0,
        mib=OPEN_MIB,
    )


def mixer_open_b(ids, x_in, taps_x, rims, step, cum, b_t, message, weight, hb, hp):
    rows, length = x_in.shape
    part = hb * HEAD_DIM

    def body(ids_ref, x_ref, tx_ref, rim_ref, step_ref, cum_ref, bt_ref, other_ref, w_ref, *outs):
        xs_ref, send_ref, mine_ref, into_ref, msg_ref, sem = outs
        copy = pltpu.make_async_copy(w_ref, into_ref, sem)
        copy.start()
        span_state(
            x_ref[part:, :], rim_ref[:, part:rows], tx_ref[:, part:], step_ref[...], cum_ref[...], bt_ref[...], xs_ref, msg_ref, hb, hp
        )
        odd = ids_ref[0] % 2 == 1
        a, b = other_ref[...].astype(F32), msg_ref[...].astype(F32)
        send_ref[...] = jnp.where(odd, a, b).astype(BF)
        mine_ref[...] = jnp.where(odd, b, a).astype(BF)
        copy.wait()

    vmem = pl.BlockSpec(memory_space=pltpu.VMEM)
    outs = [sds((part, length), BF), sds(message.shape, BF), sds(message.shape, BF), sds(weight.shape, weight.dtype)]
    return call(
        body,
        "mixer_open_b",
        ids,
        (x_in, taps_x, rims, step, cum, b_t, message, in_hbm(weight)),
        outs,
        in_specs=[vmem] * 7 + [pl.BlockSpec(memory_space=pltpu.HBM)],
        out_specs=[vmem] * len(outs),
        scratch=[pltpu.VMEM(message.shape, BF), pltpu.SemaphoreType.DMA],
        us=3.0,
        mib=OPEN_MIB,
    )


def state_pair(ids, mine, received, hb, hp):
    rows = hb * HEAD_DIM

    def body(ids_ref, mine_ref, recv_ref, msg_ref):
        odd = ids_ref[0] % 2 == 1
        t_mine, t_recv = mine_ref[:rows, :].astype(F32), recv_ref[:rows, :].astype(F32)
        d_mine, d_recv = decay_of(mine_ref, rows, hp), decay_of(recv_ref, rows, hp)
        late, early = jnp.where(odd, t_mine, t_recv), jnp.where(odd, t_recv, t_mine)
        d_late = jnp.where(odd, d_mine, d_recv)
        msg_ref[:rows, :] = (late + head_rows(d_late, hb, NSTATE) * early).astype(BF)
        high, low = sent_decay(d_mine * d_recv, hp)
        msg_ref[rows : rows + hp, :] = high
        msg_ref[rows + hp :, :] = low

    return call(body, "state_pair", ids, (mine, received), [sds(mine.shape, BF)])[0]


def state_round(ids, mine, received, carried, level, hb, hp):
    rows = hb * HEAD_DIM
    opening = carried is None
    outs = [sds(mine.shape, BF), sds((rows, NSTATE), F32), sds((hp, NSTATE), F32)]

    def body(ids_ref, mine_ref, recv_ref, *refs):
        msg_ref, pre_ref, dec_ref = refs[-3:]
        upper = (ids_ref[0] >> level) % 2 == 1
        t_mine, t_recv = mine_ref[:rows, :].astype(F32), recv_ref[:rows, :].astype(F32)
        d_mine, d_recv = decay_of(mine_ref, rows, hp), decay_of(recv_ref, rows, hp)
        late, early = jnp.where(upper, t_mine, t_recv), jnp.where(upper, t_recv, t_mine)
        d_late = jnp.where(upper, d_mine, d_recv)
        msg_ref[:rows, :] = (late + head_rows(d_late, hb, NSTATE) * early).astype(BF)
        high, low = sent_decay(d_mine * d_recv, hp)
        msg_ref[rows : rows + hp, :] = high
        msg_ref[rows + hp :, :] = low
        if opening:
            pre_ref[...] = jnp.where(upper, t_recv, jnp.zeros_like(t_recv))
            dec_ref[...] = jnp.where(upper, d_recv, jnp.ones_like(d_recv))
        else:
            old_pre, old_dec = refs[0], refs[1]
            grown = old_pre[...] + head_rows(old_dec[...], hb, NSTATE) * t_recv
            pre_ref[...] = jnp.where(upper, grown, old_pre[...])
            dec_ref[...] = jnp.where(upper, old_dec[...] * d_recv, old_dec[...])

    ins = (mine, received) if opening else (mine, received, *carried)
    return call(body, f"state_round_{level}", ids, ins, outs)


def state_finish(ids, mine, pair, carried, last, hb, hp):
    rows = hb * HEAD_DIM

    def body(ids_ref, mine_ref, pair_ref, pre_ref, dec_ref, last_ref, send_ref, keep_ref):
        odd = ids_ref[0] % 2 == 1
        before = pre_ref[...] + head_rows(dec_ref[...], hb, NSTATE) * last_ref[:rows, :].astype(F32)
        t_even = jnp.where(odd, pair_ref[:rows, :].astype(F32), mine_ref[:rows, :].astype(F32))
        d_even = jnp.where(odd, decay_of(pair_ref, rows, hp), decay_of(mine_ref, rows, hp))
        after = head_rows(d_even, hb, NSTATE) * before + t_even
        send_ref[...] = jnp.where(odd, before, after).astype(BF)
        keep_ref[...] = jnp.where(odd, after, before).astype(BF)

    outs = [sds((rows, NSTATE), BF)] * 2
    return call(body, "state_finish", ids, (mine, pair, *carried, last), outs)


def mixer_close(ids, keep, received, xs_parts, cum_parts, b_t, c_conv, z_in, gain_row, hb):
    rows, length = z_in.shape
    part = hb * HEAD_DIM
    blocks = length // BLOCK

    def body(ids_ref, keep_ref, recv_ref, xa_ref, xb_ref, ca_ref, cb_ref, bt_ref, c_ref, z_ref, gain_ref, out_ref, gram_ref, y_ref, xs_ref):
        turn = pl.program_id(0)

        @pl.when(turn == 0)
        def _():
            row = lax.broadcasted_iota(jnp.int32, (BLOCK, BLOCK), 0)
            col = lax.broadcasted_iota(jnp.int32, (BLOCK, BLOCK), 1)
            for j in range(blocks):
                span = slice(j * BLOCK, (j + 1) * BLOCK)
                gram = dot(bt_ref[span, :], c_ref[:, span])
                gram_ref[j] = jnp.where(row <= col, gram, 0.0)
            xs_ref[...] = xa_ref[...]

        @pl.when(turn == 1)
        def _():
            xs_ref[...] = xb_ref[...]

        own = turn == ids_ref[0] % 2
        state = jnp.where(own, keep_ref[...].astype(F32), recv_ref[...].astype(F32))
        cum = jnp.where(turn == 0, ca_ref[...], cb_ref[...])
        down_cum = jnp.transpose(fill_rows([cum[i : i + 1, :] for i in range(hb)]))
        before = jnp.zeros((hb, 1), F32)
        for j in range(blocks):
            span = slice(j * BLOCK, (j + 1) * BLOCK)
            here = cum[:, span]
            after = here[:, BLOCK - 1 : BLOCK]
            c_block = c_ref[:, span]
            flow = dot(state.astype(BF), c_block) * head_rows(jnp.exp(here - before), hb, BLOCK)
            gram = gram_ref[j]
            for i in range(hb):
                lines = slice(i * HEAD_DIM, (i + 1) * HEAD_DIM)
                gap = jnp.minimum(here[i : i + 1, :] - down_cum[span, i : i + 1], 0.0)
                mask = (gram * jnp.exp(gap)).astype(BF)
                y_ref[lines, span] = flow[lines, :] + dot(xs_ref[lines, span], mask)
            if j + 1 < blocks:
                fade = head_rows(jnp.exp(after - here), hb, BLOCK)
                fresh = dot((xs_ref[:, span].astype(F32) * fade).astype(BF), bt_ref[span, :])
                kept = head_rows(jnp.broadcast_to(jnp.exp(after - before), (hb, NSTATE)), hb, NSTATE)
                state = kept * state + fresh
            before = after
        gain = tall([gain_ref[:, pl.ds(pl.multiple_of(turn * part, part), part)]])
        for i in range(hb):
            lines = slice(i * HEAD_DIM, (i + 1) * HEAD_DIM)
            z_lines = pl.ds(pl.multiple_of(turn * part + i * HEAD_DIM, HEAD_DIM), HEAD_DIM)
            gated = y_ref[lines, :] * silu(z_ref[z_lines, :].astype(F32))
            scale = lax.rsqrt(jnp.mean(gated * gated, axis=0, keepdims=True) + HEAD_EPS)
            out_ref[lines, :] = (gated * scale * gain[lines, 0:1]).astype(BF)

    tile = pl.BlockSpec((part, length), lambda i, s: (i, 0))
    vmem = pl.BlockSpec(memory_space=pltpu.VMEM)
    return call(
        body,
        "mixer_close",
        ids,
        (keep, received, *xs_parts, *cum_parts, b_t, c_conv, z_in, gain_row),
        [sds((rows, length), BF)],
        grid=(2,),
        in_specs=[vmem] * 10,
        out_specs=[tile],
        scratch=[
            pltpu.VMEM((blocks, BLOCK, BLOCK), F32),
            pltpu.VMEM((part, length), F32),
            pltpu.VMEM((part, length), BF),
        ],
        us=6.0,
        mib=12,
    )[0]


def block(
    x_in,
    z_in,
    dt_raw,
    decay_rate,
    b_in,
    c_in,
    conv_x,
    conv_b,
    conv_c,
    head_gain,
    moe_rows,
    moe_gain,
    routes,
    route_logit,
    w_gate,
    w_up,
    w_down,
):
    ep, tp = lax.axis_size("ep"), lax.axis_size("tp")
    y_count = tp // 2
    heads = dt_raw.shape[0]
    hb = heads // 2
    hp = -(-hb // 16) * 16
    tokens, features = moe_rows.shape
    experts = ep * w_gate.shape[0]
    capacity = 2 * tokens * routes.shape[1] // experts
    cap = -(-capacity // 16) * 16
    sizes = (experts, cap, features // tp, y_count)
    half = experts // 2
    ids = jnp.stack([lax.axis_index("ep"), lax.axis_index("tp")]).astype(jnp.int32)
    routes_t, logit_t = routes.T, route_logit.T

    mixer_args = (
        x_in,
        b_in,
        c_in,
        dt_raw,
        decay_rate.reshape(1, -1),
        conv_x.T,
        conv_b.T,
        conv_c.T,
        head_gain.reshape(1, -1),
    )
    outs = prep(ids, moe_rows, moe_gain.reshape(1, -1), routes_t, logit_t, mixer_args, sizes)
    self_rows, near, far = outs[0], outs[1:half], outs[half : 2 * half]
    table, own_rims = outs[2 * half : 2 * half + 2]
    x_in, b_in, c_in, dt_raw, rate_row, taps_x, taps_b, taps_c, gain_row = outs[2 * half + 2 :]
    rims = lax.ppermute(own_rims, "ep", [(i, i + 1) for i in range(ep - 1)])
    far = [swap(value, "ep", half + index) for index, value in enumerate(far)]
    near = [swap(value, "ep", 1 + index) for index, value in enumerate(near)]
    far_sets = []
    for part in range(2):
        mine = far[part * half // 2 : (part + 1) * half // 2]
        value = jnp.concatenate(mine, axis=0)
        far_sets.append([value] + [swap(value, "tp", 2 * j) for j in range(1, y_count)])
    near_other = [swap(value, "tp", 1) for value in near]
    far_other = [[swap(value, "tp", 1) for value in group] for group in far_sets]

    xs_a, cum_a, cum_b, step_b, b_t, c_conv, message, w_gate = mixer_open_a(
        ids,
        x_in,
        dt_raw,
        rate_row,
        b_in,
        c_in,
        taps_x,
        taps_b,
        taps_c,
        rims,
        w_gate,
        hb,
        hp,
        y_count,
    )
    xs_b, send, mine, w_up = mixer_open_b(
        ids, x_in, taps_x, rims, step_b, cum_b, b_t, message, w_up, hb, hp
    )
    pair = swap(send, "ep", 1)
    message = state_pair(ids, mine, pair, hb, hp)
    carried, level = None, 1
    while (2 << level) < ep:
        received = swap(message, "ep", 1 << level)
        message, *carried = state_round(ids, message, received, carried, level, hb, hp)
        level += 1
    top = 1 << level
    last = lax.ppermute(message, "ep", [(i, i + top) for i in range(ep - top)])
    send, keep = state_finish(ids, mine, pair, carried, last, hb, hp)
    back = swap(send, "ep", 1)

    hid_near, hid_far, w_down, z_in = gate_up(
        ids, self_rows, near, near_other, far_sets, far_other, w_gate, w_up, w_down, z_in, sizes
    )
    send_far, keep_far = down(ids, hid_far, w_down, sizes, "down_far")
    recv_far = swap(send_far, "tp", 1)
    send_near, keep_near = down(ids, hid_near, w_down, sizes, "down_near")
    recv_near = swap(send_near, "tp", 1)
    near_out = near_sum(ids, keep_near, recv_near, sizes)
    near_back = [near_out[0]] + [swap(near_out[k], "ep", k) for k in range(1, half)]
    far_outs = far_split(ids, keep_far, recv_far, sizes)
    far_back = []
    for part in range(2):
        far_keep, *far_send = far_outs[part * y_count : (part + 1) * y_count]
        label = "ab"[part]
        far_parts = [far_keep] + [
            swap(value, "tp", 2 * (j + 1)) for j, value in enumerate(far_send)
        ]
        far_out = far_sum(ids, far_parts, sizes, "far_sum_" + label)
        first = half + part * (half // 2)
        far_back += [swap(value, "ep", first + index) for index, value in enumerate(far_out)]
    outs = near_combine(ids, near_back, table, sizes)
    near_keep = outs[0]
    near_received = [swap(value, "tp", 2 * (j + 1)) for j, value in enumerate(outs[1:])]
    moe_t = final_combine(ids, far_back, near_keep, near_received, table, sizes)

    mixed = mixer_close(
        ids,
        keep,
        back,
        (xs_a, xs_b),
        (cum_a, cum_b),
        b_t,
        c_conv,
        z_in,
        gain_row,
        hb,
    )
    return (mixed, moe_t.T)


def solution(mesh):
    return jax.shard_map(
        block,
        mesh=mesh,
        in_specs=(
            P("tp", "ep"),
            P("tp", "ep"),
            P("tp", "ep"),
            P("tp"),
            P(None, "ep"),
            P(None, "ep"),
            P("tp", None),
            P(),
            P(),
            P("tp"),
            P("ep", None),
            P(),
            P("ep", None),
            P("ep", None),
            P("ep", None, "tp"),
            P("ep", None, "tp"),
            P("ep", "tp", None),
        ),
        out_specs=(P("tp", "ep"), P("tp", "ep")),
        check_vma=False,
    )
```

```python
import jax
import jax.numpy as jnp
from jax import lax
from jax.experimental import pallas as pl
from jax.experimental.pallas import tpu as pltpu
from jax.sharding import PartitionSpec as P


HEAD_DIM = 64
GROUPS = 2
NSTATE = 128
BLOCK = 128
ROW_EPS = 0.1
HEAD_EPS = 1.0

BF = jnp.bfloat16
F32 = jnp.float32


def sds(shape, dtype):
    return jax.ShapeDtypeStruct(shape, dtype)


def dot(a, b):
    return jnp.dot(a, b, preferred_element_type=F32)


def silu(v):
    return v * (0.5 + 0.5 * jnp.tanh(0.5 * v))


def call(body, name, ids, *args, **kwargs):
    return launch(body, name, ids, *args, **kwargs)


def launch(body, name, ids, ins, outs, grid=None, in_specs=None, out_specs=None, scratch=(), us=1.0, mib=6):
    vmem = pl.BlockSpec(memory_space=pltpu.VMEM)
    common = dict(
        name=name,
        out_shape=outs,
        cost_estimate=pl.CostEstimate(
            flops=int(us * 2.5e8), bytes_accessed=0, transcendentals=0
        ),
    )
    limit = mib * 1024 * 1024
    if grid is None:
        return pl.pallas_call(
            body,
            in_specs=[pl.BlockSpec(memory_space=pltpu.SMEM)] + (in_specs or [vmem] * len(ins)),
            out_specs=out_specs or [vmem] * len(outs),
            scratch_shapes=list(scratch),
            compiler_params=pltpu.CompilerParams(vmem_limit_bytes=limit),
            **common,
        )(ids, *ins)
    return pl.pallas_call(
        body,
        grid_spec=pltpu.PrefetchScalarGridSpec(
            num_scalar_prefetch=1,
            grid=grid,
            in_specs=in_specs,
            out_specs=out_specs,
            scratch_shapes=list(scratch),
        ),
        compiler_params=pltpu.CompilerParams(
            dimension_semantics=("arbitrary",) * len(grid), vmem_limit_bytes=limit
        ),
        **common,
    )(ids, *ins)


GATE_MIB = 24
DOWN_MIB = 16
OPEN_MIB = 28


def in_hbm(value):
    return pltpu.with_memory_space_constraint(value, pltpu.HBM)


def ids_of(ids_ref):
    place, column = ids_ref[0], ids_ref[1]
    return place, column // 2, column % 2


def fill_rows(rows, count=8):
    width = rows[0].shape[1]
    at = lax.broadcasted_iota(jnp.int32, (count, width), 0)
    out = jnp.broadcast_to(rows[0], (count, width))
    for index in range(1, len(rows)):
        out = jnp.where(at == index, rows[index], out)
    return out


def destinations(routes_t, place, experts, capacity):
    tokens = routes_t.shape[1]
    relative = jnp.bitwise_xor(routes_t, place)
    first, second = relative[0:1, :], relative[1:2, :]
    at = lax.broadcasted_iota(jnp.int32, (experts, tokens), 0)
    hit_a = (at == first).astype(F32)
    hit_b = (at == second).astype(F32)
    row = lax.broadcasted_iota(jnp.int32, (tokens, tokens), 0)
    col = lax.broadcasted_iota(jnp.int32, (tokens, tokens), 1)
    before = (row < col).astype(F32).astype(BF)
    ahead = dot((hit_a + hit_b).astype(BF), before)
    rank_a = jnp.sum(hit_a * ahead, axis=0, keepdims=True).astype(jnp.int32)
    rank_b = jnp.sum(hit_b * ahead, axis=0, keepdims=True).astype(jnp.int32)
    return first * capacity + rank_a, second * capacity + rank_b


def prep(ids, moe_rows, moe_gain, routes_t, logit_t, mixer_args, sizes):
    x_in, b_in, _ = mixer_args[:3]
    tokens, features = moe_rows.shape
    experts, cap, width, y_count = sizes
    half = experts // 2
    value_rows, length = x_in.shape
    group_rows = b_in.shape[0] // GROUPS

    def body(ids_ref, rows_hbm, gain_hbm, routes_hbm, logit_hbm, *refs):
        count = len(mixer_args)
        mixer_hbm, outs, scratch = refs[:count], refs[count:-6], refs[-6:]
        normed_ref, sems = scratch[0], scratch[-1]
        rows_ref, gain_ref, routes_ref, logit_ref = scratch[1:-1]
        self_ref, near, far = outs[0], outs[1:half], outs[half : 2 * half]
        table_ref, rim_ref = outs[2 * half : 2 * half + 2]
        mixer_vmem = outs[2 * half + 2 :]
        x_ref, b_ref, c_ref = mixer_vmem[:3]
        place, y, core = ids_of(ids_ref)
        tail = slice(length - 128, length)
        moves = (
            (rows_hbm, rows_ref),
            (gain_hbm, gain_ref),
            (routes_hbm, routes_ref),
            (logit_hbm, logit_ref),
            *zip(mixer_hbm, mixer_vmem),
        )
        copies = [
            pltpu.make_async_copy(source, target, sems.at[index])
            for index, (source, target) in enumerate(moves)
        ]
        for copy in copies:
            copy.start()
        for copy in copies[:4]:
            copy.wait()
        rows = rows_ref[...].astype(F32)
        scale = lax.rsqrt(jnp.mean(rows * rows, axis=1, keepdims=True) + ROW_EPS)
        normed_ref[...] = (rows * scale * gain_ref[...]).astype(BF)
        dest_a, dest_b = destinations(routes_ref[...], place, experts, cap)

        def pick(index):
            slot = lax.broadcasted_iota(jnp.int32, (cap, tokens), 0) + index * cap
            return ((slot == dest_a) | (slot == dest_b)).astype(F32).astype(BF)

        def columns(block):
            return normed_ref[:, pl.ds(pl.multiple_of(block * width, width), width)]

        mine = columns(2 * y + core)
        for index in range(half):
            far[index][...] = dot(pick(half + index), mine).astype(BF)
        for j in range(y_count):
            part = columns(2 * j + core)
            for index in range(1, half):
                near[index - 1][:, j * width : (j + 1) * width] = dot(pick(index), part).astype(BF)
        self_ref[...] = dot(pick(0), normed_ref[...]).astype(BF)
        gap = logit_ref[0:1, :] - logit_ref[1:2, :]
        shares = [jax.nn.sigmoid(gap), jax.nn.sigmoid(-gap)]
        table_ref[...] = jnp.transpose(
            fill_rows([dest_a.astype(F32), dest_b.astype(F32)] + shares)
        )
        for copy in copies[4:]:
            copy.wait()
        group = y * (GROUPS * 2) // (2 * y_count)
        start = pl.multiple_of(group * group_rows, group_rows)
        line = lax.broadcasted_iota(jnp.int32, (16, 128), 0)
        lane = lax.broadcasted_iota(jnp.int32, (16, 128), 1)
        take = (lane == line + 125).astype(F32).astype(BF)
        nt = (((1,), (1,)), ((), ()))

        def edge(block):
            return lax.dot_general(take, block, nt, preferred_element_type=F32).astype(BF)

        rim_ref[:, :value_rows] = edge(x_ref[:, tail])
        rim_ref[:, value_rows : value_rows + group_rows] = edge(b_ref[pl.ds(start, group_rows), tail])
        rim_ref[:, value_rows + group_rows :] = edge(c_ref[pl.ds(start, group_rows), tail])

    outs = [sds((cap, features), BF)]
    outs += [sds((cap, y_count * width), BF)] * (half - 1)
    outs += [sds((cap, width), BF)] * half
    outs += [sds((tokens, 8), F32), sds((16, value_rows + 2 * group_rows), BF)]
    outs += [sds(a.shape, a.dtype) for a in mixer_args]
    return call(
        body,
        "pr",
        ids,
        tuple(map(in_hbm, (moe_rows, moe_gain, routes_t, logit_t, *mixer_args))),
        outs,
        in_specs=[pl.BlockSpec(memory_space=pltpu.HBM)] * (4 + len(mixer_args)),
        scratch=[
            pltpu.VMEM((tokens, features), BF),
            pltpu.VMEM(moe_rows.shape, BF),
            pltpu.VMEM(moe_gain.shape, F32),
            pltpu.VMEM(routes_t.shape, jnp.int32),
            pltpu.VMEM(logit_t.shape, F32),
            pltpu.SemaphoreType.DMA((4 + len(mixer_args),)),
        ],
        us=3.0,
        mib=10,
    )


def gate_up(ids, self_rows, near, near_other, far, far_other, w_gate, w_up, w_down, z_in, sizes):
    experts, cap, width, y_count = sizes
    features, hidden = w_gate.shape[1:]
    rows = experts * cap
    split = experts // 2 * cap
    step = 256 if hidden % 256 == 0 else hidden
    groups = (near, near_other, *far, *far_other)
    pieces = (self_rows, *(value for group in groups for value in group))

    def body(ids_ref, *refs):
        wg_ref, wu_ref, wd_ref, z_ref, low_ref, high_ref, held_ref, held_z_ref, lhs_ref, sems = refs[len(pieces) :]
        copies = [
            pltpu.make_async_copy(wd_ref, held_ref, sems.at[0]),
            pltpu.make_async_copy(z_ref, held_z_ref, sems.at[1]),
        ]
        for copy in copies:
            copy.start()
        at, held = 1, []
        for group in groups:
            held.append(refs[at : at + len(group)])
            at += len(group)
        _, y, core = ids_of(ids_ref)

        def columns(block):
            return pl.ds(pl.multiple_of(block * width, width), width)

        lhs_ref[0:cap, :] = refs[0][...]
        for source, c in ((held[0], core), (held[1], 1 - core)):
            for index, ref in enumerate(source):
                lines = slice(cap * (1 + index), cap * (2 + index))
                for j in range(y_count):
                    lhs_ref[lines, columns(2 * j + c)] = ref[:, j * width : (j + 1) * width]
        for set_at, c in ((2, core), (2 + len(far), 1 - core)):
            start = split
            for source in held[set_at : set_at + len(far)]:
                tall_rows = source[0].shape[0]
                for j, ref in enumerate(source):
                    lines = slice(start, start + tall_rows)
                    lhs_ref[lines, columns(2 * jnp.bitwise_xor(y, j) + c)] = ref[...]
                start += tall_rows

        for turn in range(hidden // step):
            span = slice(turn * step, (turn + 1) * step)
            for lines, out_ref in ((slice(0, split), low_ref), (slice(split, rows), high_ref)):
                lhs = lhs_ref[lines, :]
                gate = dot(lhs, wg_ref[0, :, span])
                up = dot(lhs, wu_ref[0, :, span])
                out_ref[:, span] = (silu(gate) * up).astype(BF)
        for copy in copies:
            copy.wait()

    vmem = pl.BlockSpec(memory_space=pltpu.VMEM)
    return call(
        body,
        "gu",
        ids,
        (*pieces, w_gate, w_up, in_hbm(w_down), in_hbm(z_in)),
        [sds((split, hidden), BF)] * 2 + [sds(w_down.shape, BF), sds(z_in.shape, BF)],
        in_specs=[vmem] * (len(pieces) + 2) + [pl.BlockSpec(memory_space=pltpu.HBM)] * 2,
        scratch=[pltpu.VMEM((rows, features), BF), pltpu.SemaphoreType.DMA((2,))],
        us=9.0,
        mib=GATE_MIB,
    )


def down(ids, hidden, w_down, sizes, name):
    _, _, width, y_count = sizes
    rows, _ = hidden.shape

    def body(ids_ref, h_ref, w_ref, send_ref, keep_ref):
        core = ids_ref[1] % 2
        for out_ref, c in ((send_ref, 1 - core), (keep_ref, core)):
            for j in range(y_count):
                column = pl.ds(pl.multiple_of((2 * j + c) * width, width), width)
                value = dot(h_ref[...], w_ref[0, :, column])
                out_ref[:, j * width : (j + 1) * width] = value.astype(BF)

    return call(
        body,
        name,
        ids,
        (hidden, w_down),
        [sds((rows, y_count * width), BF)] * 2,
        us=2.0,
        mib=DOWN_MIB,
    )


def near_sum(ids, keep, received, sizes):
    experts, cap, width, y_count = sizes
    half = experts // 2

    def body(ids_ref, keep_ref, recv_ref, *outs):
        for index in range(half):
            span = pl.ds(index * cap, cap)
            outs[index][...] = (
                keep_ref[span, :].astype(F32) + recv_ref[span, :].astype(F32)
            ).astype(BF)

    outs = [sds((cap, y_count * width), BF)] * half
    return call(body, "ns", ids, (keep, received), outs)


def far_split(ids, keep, received, sizes):
    _, _, width, y_count = sizes
    rows = keep.shape[0]

    def body(ids_ref, keep_ref, recv_ref, *outs):
        _, y, _ = ids_of(ids_ref)
        for part in range(2):
            lines = pl.ds(part * rows // 2, rows // 2)
            for j in range(y_count):
                column = pl.ds(pl.multiple_of(jnp.bitwise_xor(y, j) * width, width), width)
                outs[part * y_count + j][...] = (
                    keep_ref[lines, column].astype(F32) + recv_ref[lines, column].astype(F32)
                ).astype(BF)

    outs = [sds((rows // 2, width), BF)] * (2 * y_count)
    return call(body, "fs", ids, (keep, received), outs)


def far_sum(ids, parts, sizes, name):
    experts, cap, width, _ = sizes
    count = experts // 4

    def body(ids_ref, *refs):
        ins, outs = refs[: len(parts)], refs[len(parts) :]
        for index in range(count):
            span = pl.ds(index * cap, cap)
            total = ins[0][span, :].astype(F32)
            for ref in ins[1:]:
                total = total + ref[span, :].astype(F32)
            outs[index][...] = total.astype(BF)

    return call(body, name, ids, parts, [sds((cap, width), BF)] * count)


def token_weights(table, cap):
    tokens = table.shape[0]
    first, second = table[:, 0:1], table[:, 1:2]
    share_a, share_b = table[:, 2:3], table[:, 3:4]

    def pick(index):
        slot = (lax.broadcasted_iota(jnp.int32, (tokens, cap), 1) + index * cap).astype(F32)
        return (
            jnp.where(slot == first, share_a, 0.0) + jnp.where(slot == second, share_b, 0.0)
        ).astype(BF)

    return pick


def near_combine(ids, parts, table, sizes):
    _, cap, width, y_count = sizes
    tokens = table.shape[0]

    def body(ids_ref, table_ref, *refs):
        ins, outs = refs[: len(parts)], refs[len(parts) :]
        _, y, _ = ids_of(ids_ref)
        pick = token_weights(table_ref[...], cap)
        picks = [pick(index) for index in range(len(parts))]
        for j in range(y_count):
            column = pl.ds(pl.multiple_of(jnp.bitwise_xor(y, j) * width, width), width)
            total = dot(picks[0], ins[0][:, column])
            for index in range(1, len(parts)):
                total = total + dot(picks[index], ins[index][:, column])
            outs[j][...] = total.astype(outs[j].dtype)

    outs = [sds((tokens, width), F32)] + [sds((tokens, width), BF)] * (y_count - 1)
    return call(body, "nc", ids, (table, *parts), outs)


def final_combine(ids, parts, near_keep, near_received, table, sizes):
    experts, cap, width, y_count = sizes
    tokens = table.shape[0]
    half = experts // 2

    def body(ids_ref, table_ref, keep_ref, *refs):
        received, ins, out_ref = refs[: y_count - 1], refs[y_count - 1 : -1], refs[-1]
        pick = token_weights(table_ref[...], cap)
        total = keep_ref[...]
        for ref in received:
            total = total + ref[...].astype(F32)
        for index in range(half):
            total = total + dot(pick(half + index), ins[index][...])
        out_ref[...] = total.astype(BF)

    return call(
        body,
        "fc",
        ids,
        (table, near_keep, *near_received, *parts),
        [sds((tokens, width), BF)],
    )[0]


def swap(value, axis, step):
    count = lax.axis_size(axis)
    return lax.ppermute(value, axis, [(i, i ^ step) for i in range(count)])


def tall(rows):
    return jnp.transpose(fill_rows(rows))


def conv_block(signal, rim_t, taps_t):
    kinds = [taps_t[k : k + 1, :] for k in range(taps_t.shape[0])]
    taps = tall(kinds)
    count = len(kinds)
    place = lax.broadcasted_iota(jnp.int32, (16, 128), 0)
    lane = lax.broadcasted_iota(jnp.int32, (16, 128), 1)
    put = ((lane == place + 125) & (place < 3)).astype(F32).astype(BF)
    edge = dot(jnp.transpose(rim_t.astype(F32)).astype(BF), put)
    value = signal.astype(F32)
    joined = jnp.concatenate([edge, value], axis=1)
    total = taps[:, count - 1 : count] * value
    for back in range(1, count):
        total = total + taps[:, count - 1 - back : count - back] * pltpu.roll(joined, back, 1)[:, 128:]
    return silu(total)


def head_rows(table, heads_here, length):
    return jnp.concatenate(
        [jnp.broadcast_to(table[i : i + 1, :], (HEAD_DIM, length)) for i in range(heads_here)], axis=0
    )


def sent_decay(total, hp):
    count, width = total.shape
    if count < hp:
        total = jnp.concatenate([total, jnp.ones((hp - count, width), F32)], axis=0)
    high = total.astype(BF)
    return high, (total - high.astype(F32)).astype(BF)


def decay_of(ref, rows, hp):
    return ref[rows : rows + hp, :].astype(F32) + ref[rows + hp :, :].astype(F32)


def span_state(signal, rim, taps, step, cum, b_t, xs_ref, msg_ref, hb, hp):
    rows, length = signal.shape
    value = conv_block(signal, rim, taps)
    last = cum[:, length - 1 : length]
    scaled = value * head_rows(step, hb, length)
    xs_ref[...] = scaled.astype(BF)
    state = dot((scaled * head_rows(jnp.exp(last - cum), hb, length)).astype(BF), b_t)
    msg_ref[:rows, :] = state.astype(BF)
    high, low = sent_decay(jnp.broadcast_to(jnp.exp(last), (hb, NSTATE)), hp)
    msg_ref[rows : rows + hp, :] = high
    msg_ref[rows + hp :, :] = low


def mixer_open_a(ids, x_in, dt_raw, rate_row, b_in, c_in, taps_x, taps_b, taps_c, rims, weight, hb, hp, y_count):
    rows, length = x_in.shape
    heads = dt_raw.shape[0]
    part = hb * HEAD_DIM

    def body(ids_ref, x_ref, dt_ref, rate_ref, b_ref, c_ref, tx_ref, tb_ref, tc_ref, rim_ref, w_ref, *outs):
        xs_ref, cum_a_ref, cum_b_ref, step_ref, bt_ref, conv_c_ref, msg_ref, into_ref, sem = outs
        copy = pltpu.make_async_copy(w_ref, into_ref, sem)
        copy.start()
        _, y, _ = ids_of(ids_ref)
        group = y * (GROUPS * 2) // (2 * y_count)
        start = pl.multiple_of(group * NSTATE, NSTATE)
        span = pl.ds(start, NSTATE)
        b_conv = conv_block(b_ref[span, :], rim_ref[:, rows : rows + NSTATE], tb_ref[:, span])
        c_conv = conv_block(c_ref[span, :], rim_ref[:, rows + NSTATE :], tc_ref[:, span])
        b_t = jnp.transpose(b_conv).astype(BF)
        bt_ref[...] = b_t
        conv_c_ref[...] = c_conv.astype(BF)
        raw = dt_ref[...]
        step = jnp.maximum(raw, 0.0) + jnp.log1p(jnp.exp(-jnp.abs(raw)))
        eye_r = lax.broadcasted_iota(jnp.int32, (heads, heads), 0)
        eye_c = lax.broadcasted_iota(jnp.int32, (heads, heads), 1)
        rate = jnp.sum(jnp.where(eye_r == eye_c, rate_ref[...], 0.0), axis=1, keepdims=True)
        cum = -step * rate
        lane = lax.broadcasted_iota(jnp.int32, (heads, length), 1)
        shift = 1
        while shift < length:
            cum = cum + jnp.where(lane >= shift, pltpu.roll(cum, shift, 1), 0.0)
            shift *= 2
        step_ref[...] = step[hb:]
        cum_a_ref[...] = cum[:hb]
        cum_b_ref[...] = cum[hb:]
        span_state(x_ref[:part, :], rim_ref[:, :part], tx_ref[:, :part], step[:hb], cum[:hb], b_t, xs_ref, msg_ref, hb, hp)
        copy.wait()

    vmem = pl.BlockSpec(memory_space=pltpu.VMEM)
    outs = [
        sds((part, length), BF),
        sds((hb, length), F32),
        sds((hb, length), F32),
        sds((hb, length), F32),
        sds((length, NSTATE), BF),
        sds((NSTATE, length), BF),
        sds((part + 2 * hp, NSTATE), BF),
        sds(weight.shape, weight.dtype),
    ]
    return call(
        body,
        "ma",
        ids,
        (x_in, dt_raw, rate_row, b_in, c_in, taps_x, taps_b, taps_c, rims, in_hbm(weight)),
        outs,
        in_specs=[vmem] * 9 + [pl.BlockSpec(memory_space=pltpu.HBM)],
        out_specs=[vmem] * len(outs),
        scratch=[pltpu.SemaphoreType.DMA],
        us=4.0,
        mib=OPEN_MIB,
    )


def mixer_open_b(ids, x_in, taps_x, rims, step, cum, b_t, message, weight, hb, hp):
    rows, length = x_in.shape
    part = hb * HEAD_DIM

    def body(ids_ref, x_ref, tx_ref, rim_ref, step_ref, cum_ref, bt_ref, other_ref, w_ref, *outs):
        xs_ref, send_ref, mine_ref, into_ref, msg_ref, sem = outs
        copy = pltpu.make_async_copy(w_ref, into_ref, sem)
        copy.start()
        span_state(
            x_ref[part:, :], rim_ref[:, part:rows], tx_ref[:, part:], step_ref[...], cum_ref[...], bt_ref[...], xs_ref, msg_ref, hb, hp
        )
        odd = ids_ref[0] % 2 == 1
        a, b = other_ref[...].astype(F32), msg_ref[...].astype(F32)
        send_ref[...] = jnp.where(odd, a, b).astype(BF)
        mine_ref[...] = jnp.where(odd, b, a).astype(BF)
        copy.wait()

    vmem = pl.BlockSpec(memory_space=pltpu.VMEM)
    outs = [sds((part, length), BF), sds(message.shape, BF), sds(message.shape, BF), sds(weight.shape, weight.dtype)]
    return call(
        body,
        "mb",
        ids,
        (x_in, taps_x, rims, step, cum, b_t, message, in_hbm(weight)),
        outs,
        in_specs=[vmem] * 7 + [pl.BlockSpec(memory_space=pltpu.HBM)],
        out_specs=[vmem] * len(outs),
        scratch=[pltpu.VMEM(message.shape, BF), pltpu.SemaphoreType.DMA],
        us=3.0,
        mib=OPEN_MIB,
    )


def state_pair(ids, mine, received, hb, hp):
    rows = hb * HEAD_DIM

    def body(ids_ref, mine_ref, recv_ref, msg_ref):
        odd = ids_ref[0] % 2 == 1
        t_mine, t_recv = mine_ref[:rows, :].astype(F32), recv_ref[:rows, :].astype(F32)
        d_mine, d_recv = decay_of(mine_ref, rows, hp), decay_of(recv_ref, rows, hp)
        late, early = jnp.where(odd, t_mine, t_recv), jnp.where(odd, t_recv, t_mine)
        d_late = jnp.where(odd, d_mine, d_recv)
        msg_ref[:rows, :] = (late + head_rows(d_late, hb, NSTATE) * early).astype(BF)
        high, low = sent_decay(d_mine * d_recv, hp)
        msg_ref[rows : rows + hp, :] = high
        msg_ref[rows + hp :, :] = low

    return call(body, "sp", ids, (mine, received), [sds(mine.shape, BF)])[0]


def state_round(ids, mine, received, carried, level, hb, hp):
    rows = hb * HEAD_DIM
    opening = carried is None
    outs = [sds(mine.shape, BF), sds((rows, NSTATE), F32), sds((hp, NSTATE), F32)]

    def body(ids_ref, mine_ref, recv_ref, *refs):
        msg_ref, pre_ref, dec_ref = refs[-3:]
        upper = (ids_ref[0] >> level) % 2 == 1
        t_mine, t_recv = mine_ref[:rows, :].astype(F32), recv_ref[:rows, :].astype(F32)
        d_mine, d_recv = decay_of(mine_ref, rows, hp), decay_of(recv_ref, rows, hp)
        late, early = jnp.where(upper, t_mine, t_recv), jnp.where(upper, t_recv, t_mine)
        d_late = jnp.where(upper, d_mine, d_recv)
        msg_ref[:rows, :] = (late + head_rows(d_late, hb, NSTATE) * early).astype(BF)
        high, low = sent_decay(d_mine * d_recv, hp)
        msg_ref[rows : rows + hp, :] = high
        msg_ref[rows + hp :, :] = low
        if opening:
            pre_ref[...] = jnp.where(upper, t_recv, jnp.zeros_like(t_recv))
            dec_ref[...] = jnp.where(upper, d_recv, jnp.ones_like(d_recv))
        else:
            old_pre, old_dec = refs[0], refs[1]
            grown = old_pre[...] + head_rows(old_dec[...], hb, NSTATE) * t_recv
            pre_ref[...] = jnp.where(upper, grown, old_pre[...])
            dec_ref[...] = jnp.where(upper, old_dec[...] * d_recv, old_dec[...])

    ins = (mine, received) if opening else (mine, received, *carried)
    return call(body, f"q{level}", ids, ins, outs)


def state_finish(ids, mine, pair, carried, last, hb, hp):
    rows = hb * HEAD_DIM

    def body(ids_ref, mine_ref, pair_ref, pre_ref, dec_ref, last_ref, send_ref, keep_ref):
        odd = ids_ref[0] % 2 == 1
        before = pre_ref[...] + head_rows(dec_ref[...], hb, NSTATE) * last_ref[:rows, :].astype(F32)
        t_even = jnp.where(odd, pair_ref[:rows, :].astype(F32), mine_ref[:rows, :].astype(F32))
        d_even = jnp.where(odd, decay_of(pair_ref, rows, hp), decay_of(mine_ref, rows, hp))
        after = head_rows(d_even, hb, NSTATE) * before + t_even
        send_ref[...] = jnp.where(odd, before, after).astype(BF)
        keep_ref[...] = jnp.where(odd, after, before).astype(BF)

    outs = [sds((rows, NSTATE), BF)] * 2
    return call(body, "sf", ids, (mine, pair, *carried, last), outs)


def mixer_close(ids, keep, received, xs_parts, cum_parts, b_t, c_conv, z_in, gain_row, hb):
    rows, length = z_in.shape
    part = hb * HEAD_DIM
    blocks = length // BLOCK

    def body(ids_ref, keep_ref, recv_ref, xa_ref, xb_ref, ca_ref, cb_ref, bt_ref, c_ref, z_ref, gain_ref, out_ref, gram_ref, y_ref, xs_ref):
        turn = pl.program_id(0)

        @pl.when(turn == 0)
        def _():
            row = lax.broadcasted_iota(jnp.int32, (BLOCK, BLOCK), 0)
            col = lax.broadcasted_iota(jnp.int32, (BLOCK, BLOCK), 1)
            for j in range(blocks):
                span = slice(j * BLOCK, (j + 1) * BLOCK)
                gram = dot(bt_ref[span, :], c_ref[:, span])
                gram_ref[j] = jnp.where(row <= col, gram, 0.0)
            xs_ref[...] = xa_ref[...]

        @pl.when(turn == 1)
        def _():
            xs_ref[...] = xb_ref[...]

        own = turn == ids_ref[0] % 2
        state = jnp.where(own, keep_ref[...].astype(F32), recv_ref[...].astype(F32))
        cum = jnp.where(turn == 0, ca_ref[...], cb_ref[...])
        down_cum = jnp.transpose(fill_rows([cum[i : i + 1, :] for i in range(hb)]))
        before = jnp.zeros((hb, 1), F32)
        for j in range(blocks):
            span = slice(j * BLOCK, (j + 1) * BLOCK)
            here = cum[:, span]
            after = here[:, BLOCK - 1 : BLOCK]
            c_block = c_ref[:, span]
            flow = dot(state.astype(BF), c_block) * head_rows(jnp.exp(here - before), hb, BLOCK)
            gram = gram_ref[j]
            for i in range(hb):
                lines = slice(i * HEAD_DIM, (i + 1) * HEAD_DIM)
                gap = jnp.minimum(here[i : i + 1, :] - down_cum[span, i : i + 1], 0.0)
                mask = (gram * jnp.exp(gap)).astype(BF)
                y_ref[lines, span] = flow[lines, :] + dot(xs_ref[lines, span], mask)
            if j + 1 < blocks:
                fade = head_rows(jnp.exp(after - here), hb, BLOCK)
                fresh = dot((xs_ref[:, span].astype(F32) * fade).astype(BF), bt_ref[span, :])
                kept = head_rows(jnp.broadcast_to(jnp.exp(after - before), (hb, NSTATE)), hb, NSTATE)
                state = kept * state + fresh
            before = after
        gain = tall([gain_ref[:, pl.ds(pl.multiple_of(turn * part, part), part)]])
        for i in range(hb):
            lines = slice(i * HEAD_DIM, (i + 1) * HEAD_DIM)
            z_lines = pl.ds(pl.multiple_of(turn * part + i * HEAD_DIM, HEAD_DIM), HEAD_DIM)
            gated = y_ref[lines, :] * silu(z_ref[z_lines, :].astype(F32))
            scale = lax.rsqrt(jnp.mean(gated * gated, axis=0, keepdims=True) + HEAD_EPS)
            out_ref[lines, :] = (gated * scale * gain[lines, 0:1]).astype(BF)

    tile = pl.BlockSpec((part, length), lambda i, s: (i, 0))
    vmem = pl.BlockSpec(memory_space=pltpu.VMEM)
    return call(
        body,
        "mc",
        ids,
        (keep, received, *xs_parts, *cum_parts, b_t, c_conv, z_in, gain_row),
        [sds((rows, length), BF)],
        grid=(2,),
        in_specs=[vmem] * 10,
        out_specs=[tile],
        scratch=[
            pltpu.VMEM((blocks, BLOCK, BLOCK), F32),
            pltpu.VMEM((part, length), F32),
            pltpu.VMEM((part, length), BF),
        ],
        us=6.0,
        mib=12,
    )[0]


def block(
    x_in,
    z_in,
    dt_raw,
    decay_rate,
    b_in,
    c_in,
    conv_x,
    conv_b,
    conv_c,
    head_gain,
    moe_rows,
    moe_gain,
    routes,
    route_logit,
    w_gate,
    w_up,
    w_down,
):
    ep, tp = lax.axis_size("ep"), lax.axis_size("tp")
    y_count = tp // 2
    heads = dt_raw.shape[0]
    hb = heads // 2
    hp = -(-hb // 16) * 16
    tokens, features = moe_rows.shape
    experts = ep * w_gate.shape[0]
    capacity = 2 * tokens * routes.shape[1] // experts
    cap = -(-capacity // 16) * 16
    sizes = (experts, cap, features // tp, y_count)
    half = experts // 2
    ids = jnp.stack([lax.axis_index("ep"), lax.axis_index("tp")]).astype(jnp.int32)
    routes_t, logit_t = routes.T, route_logit.T

    mixer_args = (
        x_in,
        b_in,
        c_in,
        dt_raw,
        decay_rate.reshape(1, -1),
        conv_x.T,
        conv_b.T,
        conv_c.T,
        head_gain.reshape(1, -1),
    )
    outs = prep(ids, moe_rows, moe_gain.reshape(1, -1), routes_t, logit_t, mixer_args, sizes)
    self_rows, near, far = outs[0], outs[1:half], outs[half : 2 * half]
    table, own_rims = outs[2 * half : 2 * half + 2]
    x_in, b_in, c_in, dt_raw, rate_row, taps_x, taps_b, taps_c, gain_row = outs[2 * half + 2 :]
    rims = lax.ppermute(own_rims, "ep", [(i, i + 1) for i in range(ep - 1)])
    far = [swap(value, "ep", half + index) for index, value in enumerate(far)]
    near = [swap(value, "ep", 1 + index) for index, value in enumerate(near)]
    far_sets = []
    for part in range(2):
        mine = far[part * half // 2 : (part + 1) * half // 2]
        value = jnp.concatenate(mine, axis=0)
        far_sets.append([value] + [swap(value, "tp", 2 * j) for j in range(1, y_count)])
    near_other = [swap(value, "tp", 1) for value in near]
    far_other = [[swap(value, "tp", 1) for value in group] for group in far_sets]

    xs_a, cum_a, cum_b, step_b, b_t, c_conv, message, w_gate = mixer_open_a(
        ids,
        x_in,
        dt_raw,
        rate_row,
        b_in,
        c_in,
        taps_x,
        taps_b,
        taps_c,
        rims,
        w_gate,
        hb,
        hp,
        y_count,
    )
    xs_b, send, mine, w_up = mixer_open_b(
        ids, x_in, taps_x, rims, step_b, cum_b, b_t, message, w_up, hb, hp
    )
    pair = swap(send, "ep", 1)
    message = state_pair(ids, mine, pair, hb, hp)
    carried, level = None, 1
    while (2 << level) < ep:
        received = swap(message, "ep", 1 << level)
        message, *carried = state_round(ids, message, received, carried, level, hb, hp)
        level += 1
    top = 1 << level
    last = lax.ppermute(message, "ep", [(i, i + top) for i in range(ep - top)])
    send, keep = state_finish(ids, mine, pair, carried, last, hb, hp)
    back = swap(send, "ep", 1)

    hid_near, hid_far, w_down, z_in = gate_up(
        ids, self_rows, near, near_other, far_sets, far_other, w_gate, w_up, w_down, z_in, sizes
    )
    send_far, keep_far = down(ids, hid_far, w_down, sizes, "df")
    recv_far = swap(send_far, "tp", 1)
    send_near, keep_near = down(ids, hid_near, w_down, sizes, "dn")
    recv_near = swap(send_near, "tp", 1)
    near_out = near_sum(ids, keep_near, recv_near, sizes)
    near_back = [near_out[0]] + [swap(near_out[k], "ep", k) for k in range(1, half)]
    far_outs = far_split(ids, keep_far, recv_far, sizes)
    far_back = []
    for part in range(2):
        far_keep, *far_send = far_outs[part * y_count : (part + 1) * y_count]
        label = "ab"[part]
        far_parts = [far_keep] + [
            swap(value, "tp", 2 * (j + 1)) for j, value in enumerate(far_send)
        ]
        far_out = far_sum(ids, far_parts, sizes, "t" + label)
        first = half + part * (half // 2)
        far_back += [swap(value, "ep", first + index) for index, value in enumerate(far_out)]
    outs = near_combine(ids, near_back, table, sizes)
    near_keep = outs[0]
    near_received = [swap(value, "tp", 2 * (j + 1)) for j, value in enumerate(outs[1:])]
    moe_t = final_combine(ids, far_back, near_keep, near_received, table, sizes)

    mixed = mixer_close(
        ids,
        keep,
        back,
        (xs_a, xs_b),
        (cum_a, cum_b),
        b_t,
        c_conv,
        z_in,
        gain_row,
        hb,
    )
    return (mixed, moe_t.T)


def solution(mesh):
    return jax.shard_map(
        block,
        mesh=mesh,
        in_specs=(
            P("tp", "ep"),
            P("tp", "ep"),
            P("tp", "ep"),
            P("tp"),
            P(None, "ep"),
            P(None, "ep"),
            P("tp", None),
            P(),
            P(),
            P("tp"),
            P("ep", None),
            P(),
            P("ep", None),
            P("ep", None),
            P("ep", None, "tp"),
            P("ep", None, "tp"),
            P("ep", "tp", None),
        ),
        out_specs=(P("tp", "ep"), P("tp", "ep")),
        check_vma=False,
    )
```
